256 devices in a mesh: sp: 32 (over z, x), tp: 8 (over y, core).
Axes of the slice: x: 4, y: 4, z: 8, core: 2. Of those that a mesh axis runs over, the one named last changes fastest.
Arguments:
- inputs: bfloat16 [12288, 2048], P('sp', 'tp'), may hold values from -6 to 6
- norm_gain: float32 [2048], replicated, may hold values from 0.1 to 1.9
- query_weight: bfloat16 [2048, 1024], P(None, 'tp')
- key_weight: bfloat16 [2048, 1024], P(None, 'tp'), may hold values from -0.15625 to 0.15625
- value_weight: bfloat16 [2048, 1024], P(None, 'tp'), may hold values from -0.125 to 0.125
- memory_query_weight: bfloat16 [2048, 1024], P(None, 'tp'), may hold values from -0.125 to 0.125
- memory_key_weight: bfloat16 [2048, 1024], P(None, 'tp'), may hold values from -0.125 to 0.125
- memory_value_weight: bfloat16 [2048, 1024], P(None, 'tp'), may hold values from -0.125 to 0.125
- input_gate_weight: bfloat16 [2048, 16], P(None, 'tp')
- forget_gate_weight: bfloat16 [2048, 16], P(None, 'tp'), may hold values from -0.3125 to 0.3125
- forget_bias: float32 [16], P('tp'), may hold values from 3 to 13
- decay_shift: float32 [12288, 16], P('sp', 'tp'), may hold values from -2 to 0, as said below
- lambdas: float32 [16], P('tp'), may hold values from 0.3 to 0.8
- head_gain: float32 [64], replicated, may hold values from 0.1 to 1.9
- out_weight_attention: bfloat16 [1024, 2048], P('tp'), may hold values from -0.125 to 0.125
- out_weight_memory: bfloat16 [1024, 2048], P('tp'), may hold values from -0.125 to 0.125
Outputs:
- combined: bfloat16 [12288, 2048], P('sp', 'tp')
The draws below stay inside these ranges and needn't reach their ends.
Inputs may be any that keep to these rules, and one draw needn't show every extreme that they name: `decay_shift`: never positive.
All inputs are finite; a program needn't handle non-finite values.
Results may differ from the reference program's by a relative error of at most 0.018.
The reference program's roundings to bfloat16 on the way count: a program that leaves them out, or rounds other values in their place, can miss the bound.
Values may be sent and summed in bfloat16 or wider, within the bound.
A program may use at most 192 MiB of HBM per device.

```python
import math
import jax
import jax.numpy as jnp
from jax import lax

D = 2048
HEAD = 64
DD = 32
HD = 16
MATRIX_HEADS = 16
BLOCK = 64
SEQUENCE_TOKENS = 12288
N_TP = 8


def draw_query_weight(key, part):
    entries = jnp.clip(jax.random.normal(jax.random.fold_in(key, 11), (D, HD * HEAD), jnp.float32), -6.0, 6.0)
    entries = entries * (1.3 / D ** 0.5)
    return entries.astype(jnp.bfloat16)


def draw_input_gate_weight(key, part):
    entries = jnp.clip(jax.random.normal(jax.random.fold_in(key, 13), (D, MATRIX_HEADS), jnp.float32), -6.0, 6.0)
    entries = entries / D ** 0.5
    return entries.astype(jnp.bfloat16)


def draw_forget_bias(key, part):
    fast_share = 0.5
    fast_heads = jax.random.uniform(jax.random.fold_in(key, 21), (MATRIX_HEADS,), jnp.float32) < fast_share
    jitter = jax.random.uniform(jax.random.fold_in(key, 22), (MATRIX_HEADS,), jnp.float32)
    quick_bias = math.log(40.0) + jitter - 0.5
    slow_bias = math.log(float(SEQUENCE_TOKENS)) + 2.0 + jitter
    return jnp.where(fast_heads, quick_bias, slow_bias).astype(jnp.float32)


def draw_decay_shift(key, part):
    block_count = SEQUENCE_TOKENS // BLOCK
    factor = jnp.exp(jax.random.uniform(jax.random.fold_in(key, 31), (block_count, 1, MATRIX_HEADS), jnp.float32, math.log(0.3), math.log(5.0)))
    constant_level = -jnp.broadcast_to(factor, (block_count, BLOCK, MATRIX_HEADS)).reshape(SEQUENCE_TOKENS, MATRIX_HEADS) / SEQUENCE_TOKENS
    spike_row_list = jax.random.randint(jax.random.fold_in(key, 32), (4, MATRIX_HEADS), 0, SEQUENCE_TOKENS)
    spike_dropouts = jnp.log(jax.random.uniform(jax.random.fold_in(key, 33), (4, MATRIX_HEADS), jnp.float32, 0.4, 0.75))
    row_indices = jnp.arange(SEQUENCE_TOKENS, dtype=jnp.int32)[:, None, None]
    spike_events = jnp.sum(jnp.where(row_indices == spike_row_list[None], spike_dropouts[None], 0.0), axis=1)
    return jnp.maximum(constant_level + spike_events, -2.0).astype(jnp.float32)


def levels(own_key, extent, cuts, low, top_value):
    def one(position, parts):
        draws = jax.random.uniform(jax.random.fold_in(jax.random.fold_in(own_key, 6), position), (parts,), jnp.float32, low / len(cuts), top_value / len(cuts))
        return jnp.repeat(jnp.exp(draws), extent[position] // parts).reshape((-1,) + (1,) * (len(extent) - position - 1))

    gain = one(*cuts[0])
    for cut in cuts[1:]:
        gain = gain * one(*cut)
    return gain


def centred(own_key, extent, deviation, bound, shards=(), kind=jnp.bfloat16):
    drawn = deviation * jax.random.normal(own_key, extent, jnp.float32)
    if shards:
        drawn = drawn * levels(own_key, extent, shards, -0.22, 0.18)
    return jnp.clip(drawn, -bound, bound).astype(kind)


def setup_inputs(seed: int = 0) -> dict:
    key_of = jax.random.split(jax.random.key(seed), 17)
    return {
        "inputs": centred(key_of[0], (SEQUENCE_TOKENS, D), 1.0, 6.0, ((0, 32), (1, 8))),
        "norm_gain": jnp.clip(1.0 + 0.18 * jax.random.normal(key_of[1], (D,), jnp.float32), 0.1, 1.9),
        "query_weight": draw_query_weight(jax.random.fold_in(key_of[16], 71), 0),
        "key_weight": centred(key_of[3], (D, HD * HEAD), (D * 10 // 17) ** -0.5, 0.15625, ((1, 8),)),
        "value_weight": centred(key_of[4], (D, HD * HEAD), D ** -0.5, 0.125, ((1, 8),)),
        "memory_query_weight": centred(key_of[5], (D, MATRIX_HEADS * HEAD), D ** -0.5, 0.125, ((1, 8),)),
        "memory_key_weight": centred(key_of[6], (D, MATRIX_HEADS * HEAD), D ** -0.5, 0.125, ((1, 8),)),
        "memory_value_weight": centred(key_of[7], (D, MATRIX_HEADS * HEAD), D ** -0.5, 0.125, ((1, 8),)),
        "input_gate_weight": draw_input_gate_weight(jax.random.fold_in(key_of[16], 71), 0),
        "forget_gate_weight": centred(key_of[9], (D, MATRIX_HEADS), (D // 6) ** -0.5, 0.3125, ((1, 8),)),
        "forget_bias": draw_forget_bias(jax.random.fold_in(key_of[16], 71), 0),
        "decay_shift": draw_decay_shift(jax.random.fold_in(key_of[16], 71), 0),
        "lambdas": jnp.clip(0.3 + 0.5 * jax.random.uniform(key_of[12], (HD,), jnp.float32) ** levels(key_of[12], (HD,), ((0, 8),), -0.2, 0.2), 0.3, 0.8),
        "head_gain": jnp.clip(1.0 + 0.18 * jax.random.normal(key_of[13], (HEAD,), jnp.float32), 0.1, 1.9),
        "out_weight_attention": centred(key_of[14], (HD * HEAD, D), ((HD + MATRIX_HEADS) * HEAD) ** -0.5, 0.125, ((0, 8),)),
        "out_weight_memory": centred(key_of[15], (MATRIX_HEADS * HEAD, D), ((HD + MATRIX_HEADS) * HEAD) ** -0.5, 0.125, ((0, 8),)),
    }


EPSILON = 1e-06
ROTARY_BASE = 10000.0
NEGATIVE = -1e+30

def rotate(halves, positions):
    middle = halves.shape[-1] // 2
    inverse = 1.0 / ROTARY_BASE ** (jnp.arange(middle, dtype=jnp.float32) / middle)
    angles = positions.astype(jnp.float32)[:, None] * inverse[None, :]
    cosine = jnp.cos(angles)[:, None, :]
    sine_part = jnp.sin(angles)[:, None, :]
    floats = halves.astype(jnp.float32)
    former = floats[..., :middle]
    latter = floats[..., middle:]
    turned = jnp.concatenate([former * cosine - latter * sine_part, latter * cosine + former * sine_part], axis=-1)
    return turned.astype(jnp.bfloat16)

def advance_state(carried, block_entry):
    memory, normal, stable = carried
    block_memory, block_normal, block_max, block_decay = block_entry
    new_stable = jnp.maximum(block_decay + stable, block_max)
    former = jnp.exp(block_decay + stable - new_stable)
    latter = jnp.exp(block_max - new_stable)
    return (former[:, None, None] * memory + latter[:, None, None] * block_memory, former[:, None] * normal + latter[:, None] * block_normal, new_stable)

def memory_blocks(queries, key_heads, values, gate_in, log_forget, entering):
    token_count, head_count, head_width = queries.shape
    block_count = token_count // BLOCK
    highest = lax.Precision.HIGHEST

    def blocked(flat_array):
        return flat_array.astype(jnp.float32).reshape(block_count, BLOCK, head_count, head_width).transpose(2, 0, 1, 3)
    query_blocks = blocked(queries)
    key_blocks = blocked(key_heads) * head_width ** (-0.5)
    value_blocks = blocked(values)
    gate_blocks = gate_in.reshape(block_count, BLOCK, head_count).transpose(2, 0, 1)
    cumulative = jnp.cumsum(log_forget.reshape(block_count, BLOCK, head_count).transpose(2, 0, 1), axis=-1)
    block_ends = cumulative[..., -1]
    toward_end = block_ends[..., None] - cumulative + gate_blocks
    local_max = lax.optimization_barrier(jnp.max(toward_end, axis=-1))
    end_weights = jnp.exp(toward_end - local_max[..., None])
    local_memory = jnp.einsum('hcl,hclv,hclk->chvk', end_weights, value_blocks, key_blocks, precision=highest)
    local_normal = jnp.einsum('hcl,hclk->chk', end_weights, key_blocks, precision=highest)

    def scan_step(carried, block_entry):
        return (advance_state(carried, block_entry), carried)
    entries = (local_memory, local_normal, local_max.T, block_ends.T)
    unused, (memory_in, normal_in, stable_in) = lax.scan(scan_step, entering, entries)
    lower_mask = jnp.tril(jnp.ones((BLOCK, BLOCK), dtype=bool))
    decays = jnp.where(lower_mask, cumulative[..., :, None] - cumulative[..., None, :] + gate_blocks[..., None, :], NEGATIVE)
    carried_log = cumulative + stable_in.T[..., None]
    row_max = jnp.maximum(carried_log, lax.optimization_barrier(jnp.max(decays, axis=-1)))
    within = jnp.where(lower_mask, jnp.exp(decays - row_max[..., None]), 0.0)
    outside = jnp.exp(carried_log - row_max)
    scores = within * jnp.einsum('hctd,hcsd->hcts', query_blocks, key_blocks, precision=highest)
    numerator = outside[..., None] * jnp.einsum('chvk,hctk->hctv', memory_in, query_blocks, precision=highest)
    numerator = numerator + jnp.einsum('hcts,hcsv->hctv', scores, value_blocks, precision=highest)
    denominator = outside * jnp.einsum('chk,hctk->hct', normal_in, query_blocks, precision=highest) + lax.optimization_barrier(jnp.sum(scores, axis=-1))
    result = numerator / jnp.maximum(jnp.abs(denominator), 1.0)[..., None]
    return result.transpose(1, 2, 0, 3).reshape(token_count, head_count * head_width).astype(jnp.bfloat16)

def differential(query_first, query_second, key_first, key_second, values, lambdas, head_gain):
    token_count = query_first.shape[0]
    query_span = min(512, token_count)
    score_scale = DD ** (-0.5)
    key_positions = jnp.arange(token_count, dtype=jnp.int32)

    def per_head(head_entry):
        head_query_first, head_query_second, head_key_first, head_key_second, value_head, factor = head_entry

        def per_block(block_index):
            first_row = block_index * query_span
            query_positions = first_row + jnp.arange(query_span, dtype=jnp.int32)
            visible = key_positions[None, :] <= query_positions[:, None]
            results = []
            for query_side, key_side in ((head_query_first, head_key_first), (head_query_second, head_key_second)):
                query_block = lax.dynamic_slice_in_dim(query_side, first_row, query_span, 0)
                scores = jnp.dot(query_block, key_side.T, preferred_element_type=jnp.float32) * score_scale
                scores = jnp.where(visible, scores, NEGATIVE)
                row_max = lax.optimization_barrier(jnp.max(scores, axis=1, keepdims=True))
                weights = jnp.where(visible, jnp.exp(scores - row_max), 0.0)
                totals = lax.optimization_barrier(jnp.sum(weights, axis=1, keepdims=True))
                results.append(jnp.dot(weights.astype(jnp.bfloat16), value_head, preferred_element_type=jnp.float32) / totals)
            return results[0] - factor * results[1]
        return lax.map(per_block, jnp.arange(token_count // query_span, dtype=jnp.int32))
    entries = (query_first.transpose(1, 0, 2), query_second.transpose(1, 0, 2), key_first.transpose(1, 0, 2), key_second.transpose(1, 0, 2), values.transpose(1, 0, 2), lambdas)
    stacked = lax.map(per_head, entries)
    head_count = stacked.shape[0]
    stacked = stacked.reshape(head_count, token_count, -1).transpose(1, 0, 2)
    norm_scale = lax.rsqrt(lax.optimization_barrier(jnp.mean(stacked * stacked, axis=-1, keepdims=True)) + EPSILON)
    return (stacked * norm_scale * head_gain).astype(jnp.bfloat16).reshape(token_count, -1)

def reference(inputs, norm_gain, query_weight, key_weight, value_weight, memory_query_weight, memory_key_weight, memory_value_weight, input_gate_weight, forget_gate_weight, forget_bias, decay_shift, lambdas, head_gain, out_weight_attention, out_weight_memory):
    token_count = inputs.shape[0]
    floats = inputs.astype(jnp.float32)
    inverse_rms = lax.rsqrt(lax.optimization_barrier(jnp.mean(floats * floats, axis=1, keepdims=True)) + EPSILON)
    scaled = (floats * norm_gain[None, :]).astype(jnp.bfloat16)

    def project(weight):
        return jnp.dot(scaled, weight, preferred_element_type=jnp.float32) * inverse_rms

    def split_heads(weight):
        return project(weight).astype(jnp.bfloat16).reshape(token_count, -1, HEAD)
    positions = jnp.arange(token_count, dtype=jnp.int32)
    queries = split_heads(query_weight)
    key_heads = split_heads(key_weight)
    values = split_heads(value_weight)
    attended = differential(rotate(queries[..., :DD], positions), rotate(queries[..., DD:], positions), rotate(key_heads[..., :DD], positions), rotate(key_heads[..., DD:], positions), values, lambdas, head_gain)
    gate_in = project(input_gate_weight)
    log_forget = jax.nn.log_sigmoid(project(forget_gate_weight) + forget_bias[None, :]) + decay_shift
    head_count = gate_in.shape[1]
    entering = (jnp.zeros((head_count, HEAD, HEAD), jnp.float32), jnp.zeros((head_count, HEAD), jnp.float32), jnp.zeros((head_count,), jnp.float32))
    memory = memory_blocks(split_heads(memory_query_weight), split_heads(memory_key_weight), split_heads(memory_value_weight), gate_in, log_forget, entering)
    attended_width = attended.shape[1] // N_TP
    memory_width = memory.shape[1] // N_TP
    combined = jnp.zeros((token_count, out_weight_attention.shape[1]), jnp.float32)
    for group_index in range(N_TP):
        low_a = group_index * attended_width
        low_m = group_index * memory_width
        partial_sum = jnp.dot(attended[:, low_a:low_a + attended_width], out_weight_attention[low_a:low_a + attended_width], preferred_element_type=jnp.float32)
        partial_sum = partial_sum + jnp.dot(memory[:, low_m:low_m + memory_width], out_weight_memory[low_m:low_m + memory_width], preferred_element_type=jnp.float32)
        combined = combined + lax.optimization_barrier(partial_sum.astype(jnp.bfloat16)).astype(jnp.float32)
    return combined.astype(jnp.bfloat16)
```

```python
import jax
import jax.numpy as jnp
from jax import lax
from jax.experimental import pallas as pl
from jax.experimental.pallas import tpu as pltpu
from jax.sharding import PartitionSpec as P

HEAD = 64
DD = 32
EPSILON = 1e-06
ROTARY_BASE = 10000.0
NEGATIVE = -1e30
LOG2E = 1.4426950408889634
SPANS = 32
ROUNDS = 5
CHUNKS = 4
MESH = pl.DeviceIdType.MESH
F32 = jnp.float32
BF16 = jnp.bfloat16


def ring_position(ring, span):
    a, b = span // 4, span % 4
    if ring == 0:
        return 4 * a + (a + b) % 4
    r = (a + 5 * b) % 8
    return 4 * (b + 4 * (r // 4)) + r % 4


def span_on_ring(ring, position):
    u, r = position // 4, position % 4
    if ring == 0:
        return 4 * u + (r + 32 - u) % 4
    return 4 * ((3 * u + r) % 8) + u % 4


def dot(a, b):
    return jnp.dot(a, b, preferred_element_type=F32)


def dot_t(a, b):
    return lax.dot_general(a, b, (((1,), (1,)), ((), ())), preferred_element_type=F32)


def halves(a):
    high = a.astype(BF16)
    return high, (a - high.astype(F32)).astype(BF16)


def thirds(a):
    high = a.astype(BF16)
    rest = a - high.astype(F32)
    middle = rest.astype(BF16)
    return high, middle, (rest - middle.astype(F32)).astype(BF16)


def layer_kernel(
    x, gain, cosine, sine, wq, wk, wv, wmq, wmk, wmv, wig, wfg, bias, decay, lambdas, head_gain,
    woa, wom, out,
    xg, xs, squares, w, wi, wf, wo, held, qs, mq, mk, mv, gates, acc, top, st_in, st_out, st_before,
    num_local, log_local, cat, to_partner, from_partner, to_ring, from_ring,
    load_sem, gather_send, gather_recv, ring_send, ring_recv, scan_send, scan_recv,
    pair_send, pair_recv, sum_send, sum_recv,
):
    rows = x.shape[0]
    half_rows = rows // 2
    chunk = rows // CHUNKS
    sp = lax.axis_index("sp")
    tp = lax.axis_index("tp")
    y, c = tp // 2, tp % 2
    right = 2 * ((y + 1) % 4) + c
    left = 2 * ((y + 3) % 4) + c
    across = 2 * ((y + 2) % 4) + c
    partner = 2 * y + 1 - c
    t0, t1 = ring_position(0, sp), ring_position(1, sp)
    nexts = [span_on_ring(ring, (t + step) % SPANS)
             for ring, t in ((0, t0), (1, t1)) for step in (1, SPANS - 1)]

    def remote(src, dst, send, recv, span, seat):
        return pltpu.make_async_remote_copy(
            src_ref=src, dst_ref=dst, send_sem=send, recv_sem=recv,
            device_id=(span, seat), device_id_type=MESH)

    own_load = pltpu.make_async_copy(x, xg.at[tp], load_sem.at[0])
    own_load.start()
    loads = []
    for number, (weight, tile, at) in enumerate(
            ((wq, 0, 0), (wk, 0, 128), (wv, 1, 0), (wmq, 1, 128), (wmk, 2, 0), (wmv, 2, 128))):
        loads.append(pltpu.make_async_copy(
            weight, w.at[tile, :, pl.ds(at, 128)], load_sem.at[1 + number]))
    loads.append(pltpu.make_async_copy(wig, wi, load_sem.at[7]))
    loads.append(pltpu.make_async_copy(wfg, wf, load_sem.at[8]))
    for load in loads:
        load.start()
    out_loads = []
    for j in range(8):
        for part, weight in enumerate((woa, wom)):
            out_loads.append(pltpu.make_async_copy(
                weight.at[:, pl.ds(256 * j, 256)], wo.at[j, pl.ds(128 * part, 128), :],
                load_sem.at[9 + 2 * j + part]))
    for load in out_loads:
        load.start()

    barrier = pltpu.get_barrier_semaphore()
    greeted = [(sp, right), (sp, left), (sp, partner)] + [(span, tp) for span in nexts]
    for number in range(ROUNDS):
        greeted.append(((sp + 2 ** number) % SPANS, tp))
        if number < ROUNDS - 1:
            greeted.append(((sp + SPANS - 2 ** number) % SPANS, tp))
    for span, seat in greeted:
        pl.semaphore_signal(barrier, inc=1, device_id=(span, seat), device_id_type=MESH)
    pl.semaphore_wait(barrier, len(greeted))

    def piece(seat, half):
        return xg.at[seat, pl.ds(half * half_rows, half_rows), :]

    def gather(number, ref, seat):
        return remote(ref, ref, gather_send.at[number], gather_recv.at[number], sp, seat)

    sends = {
        0: gather(0, piece(tp, 0), right),
        1: gather(1, piece(tp, 1), right),
        2: gather(2, piece(tp, 1), left),
        3: gather(3, piece(tp, 0), left),
        4: gather(4, xg.at[tp], partner),
        5: gather(5, piece(left, 0), right),
        6: gather(6, piece(left, 0), partner),
        7: gather(7, piece(right, 1), left),
        8: gather(8, piece(right, 1), partner),
        9: gather(9, piece(left, 1), partner),
        10: gather(10, piece(right, 0), partner),
        11: gather(11, piece(across, 0), partner),
        12: gather(12, piece(across, 1), partner),
    }
    own_load.wait()
    for number in (0, 2, 1, 3, 4):
        sends[number].start()

    def absorb(seat):
        block = xg[seat].astype(F32)
        squares[...] += block * block
        xs[seat] = (block * gain[seat]).astype(BF16)

    squares[...] = jnp.zeros_like(squares)
    absorb(tp)
    sends[0].wait_recv()
    sends[5].start()
    sends[6].start()
    sends[2].wait_recv()
    sends[7].start()
    sends[8].start()
    sends[4].wait_recv()
    absorb(partner)
    sends[1].wait_recv()
    sends[9].start()
    sends[3].wait_recv()
    sends[10].start()
    absorb(left)
    absorb(right)
    sends[5].wait_recv()
    sends[11].start()
    sends[7].wait_recv()
    sends[12].start()
    for number in (6, 8, 9, 10):
        sends[number].wait_recv()
    absorb(2 * ((y + 1) % 4) + 1 - c)
    absorb(2 * ((y + 3) % 4) + 1 - c)
    absorb(across)
    sends[11].wait_recv()
    sends[12].wait_recv()
    absorb(2 * ((y + 2) % 4) + 1 - c)
    for number in range(13):
        sends[number].wait_send()
    for load in loads:
        load.wait()

    inverse = lax.rsqrt(
        jnp.sum(squares[...], axis=1, keepdims=True) * (1.0 / 2048.0) + EPSILON)
    scaled = jnp.concatenate([xs[j] for j in range(8)], axis=1)
    lane = lax.broadcasted_iota(jnp.int32, (rows, 128), 1)
    low = lane < HEAD
    former = lane % 32 < 16

    def rotated(flat):
        floats = flat.astype(BF16).astype(F32)
        swapped = jnp.where(former, pltpu.roll(floats, 112, 1), pltpu.roll(floats, 16, 1))
        return (floats * cosine[...] + swapped * sine[...]).astype(BF16).astype(F32)

    product = dot(scaled, w[0]) * inverse
    queries = rotated(product[:, :128])
    keys = rotated(product[:, 128:])
    product = dot(scaled, w[1]) * inverse
    values = product[:, :128].astype(BF16).astype(F32)
    mq[...] = product[:, 128:].astype(BF16)
    held[0, t0] = jnp.where(low, keys, pltpu.roll(values, 64, 1)).astype(BF16)
    held[1, t1] = jnp.where(low, pltpu.roll(keys, 64, 1), values).astype(BF16)
    for head in range(2):
        turned = queries if head == 0 else pltpu.roll(queries, 64, 1)
        for side in range(2):
            inside = (lane >= DD * side) & (lane < DD * side + DD)
            qs[head, side * rows:(side + 1) * rows, :] = jnp.where(inside, turned, 0.0).astype(BF16)

    def passing(stream, step, number):
        ring, way = stream // 2, stream % 2
        t = (t0, t1)[ring]
        origin = (t + SPANS - step) % SPANS if way == 0 else (t + step) % SPANS
        ref = held.at[ring, origin, pl.ds(number * chunk, chunk), :]
        return remote(ref, ref, ring_send.at[stream, number],
                      ring_recv.at[stream, step, number], nexts[stream], tp)

    for number in range(CHUNKS):
        for stream in range(4):
            passing(stream, 0, number).start()

    product = dot(scaled, w[2]) * inverse
    mk[...] = product[:, :128].astype(BF16)
    mv[...] = product[:, 128:].astype(BF16)
    gate_in = dot(scaled, wi[...]) * inverse
    forget = dot(scaled, wf[...]) * inverse

    def log_sigmoid(a):
        return jnp.minimum(a, 0.0) - jnp.log1p(jnp.exp(-jnp.abs(a)))

    def per_head(parts):
        return jnp.where(low, parts[0], parts[1])

    log_forget = per_head([
        log_sigmoid(forget[:, h:h + 1] + bias[h]) + decay[:, h:h + 1] for h in range(2)])
    gate = per_head([gate_in[:, h:h + 1] for h in range(2)])
    before_or_at = (lax.broadcasted_iota(jnp.int32, (rows, rows), 1)
                    <= lax.broadcasted_iota(jnp.int32, (rows, rows), 0))
    triangle = jnp.where(before_or_at, 1.0, 0.0).astype(BF16)
    high, middle, small = thirds(log_forget)
    cumulative = dot(triangle, high) + dot(triangle, middle) + dot(triangle, small)
    gates[0] = cumulative
    gates[1] = gate - cumulative
    span_decay = cumulative[rows - 1:rows, :]
    toward_end = span_decay + gates[1]
    span_top = jnp.max(toward_end, axis=0, keepdims=True)
    end_weights = jnp.exp(toward_end - span_top)
    key_floats = mk[...].astype(F32) * 0.125
    weighted = jnp.transpose(end_weights * mv[...].astype(F32))
    high, small = halves(weighted)
    keys_exact = key_floats.astype(BF16)
    outer = dot(high, keys_exact) + dot(small, keys_exact)
    row = lax.broadcasted_iota(jnp.int32, (8, 128), 0)

    def tail(normal, stable, decays):
        return jnp.where(row == 0, normal, jnp.where(row == 1, stable, decays))

    low_square = low[:HEAD]
    st_out[0, 0:HEAD, :] = jnp.where(low_square, outer[:HEAD], outer[HEAD:])
    st_out[0, HEAD:HEAD + 8, :] = tail(
        jnp.sum(end_weights * key_floats, axis=0, keepdims=True), span_top, span_decay)
    st_before[0:HEAD, :] = jnp.zeros((HEAD, 128), F32)
    st_before[HEAD:HEAD + 8, :] = tail(0.0, NEGATIVE, 0.0) + jnp.zeros((8, 128), F32)

    def scan_copy(number):
        target = (sp + lax.shift_left(jnp.int32(1), jnp.int32(number))) % SPANS
        return remote(st_out.at[number], st_in.at[number], scan_send.at[number],
                      scan_recv.at[number], target, tp)

    def joined(earlier, later):
        old, new = earlier[1], later[1]
        decays, stable, later_stable = new[2:3], old[1:2], new[1:2]
        highest = jnp.maximum(decays + stable, later_stable)
        first = jnp.exp(decays + stable - highest)
        second = jnp.exp(later_stable - highest)
        return (first * earlier[0] + second * later[0],
                tail(first * old[0:1] + second * new[0:1], highest, old[2:3] + decays))

    scale = DD ** (-0.5) * LOG2E
    ones_low = low

    def visit(ring, position, mask=None):
        block = held[ring, position]
        extended = jnp.where(ones_low, jnp.ones_like(block), block)
        scores = dot_t(qs[ring], block)
        if mask is not None:
            scores = jnp.where(mask, scores, NEGATIVE)
            highest = jnp.broadcast_to(jnp.max(scores, axis=1, keepdims=True), (2 * rows, 128))
        else:
            old = top[ring]
            highest = jnp.maximum(old, jnp.max(scores, axis=1, keepdims=True))
        shift = highest * scale
        weights = jnp.exp2(scores * scale - jnp.concatenate([shift] * (rows // 128), axis=1))
        product = dot(weights.astype(BF16), extended)
        if mask is not None:
            acc[ring] = product
        else:
            acc[ring] = acc[ring] * jnp.exp2((old - highest) * scale) + product
        top[ring] = highest

    causal = jnp.concatenate([before_or_at, before_or_at], axis=0)
    visit(0, t0, causal)
    scan_copy(0).start()
    visit(1, t1, causal)

    def local_memory():
        sums, tops, totals = [], [], []
        turned = jnp.transpose(gates[1])
        for head in range(2):
            inside = low if head == 0 else ~low
            gap = gates[0][:, HEAD * head:HEAD * head + 1] + turned[HEAD * head:HEAD * head + 1, :]
            gap = jnp.where(before_or_at, gap, NEGATIVE)
            highest = jnp.max(gap, axis=1, keepdims=True)
            within = jnp.exp(gap - highest)
            mine = jnp.where(inside, mq[...].astype(F32), 0.0).astype(BF16)
            scores = within * (dot_t(mine, mk[...]) * 0.125)
            high, small = halves(scores)
            sums.append(dot(high, mv[...]) + dot(small, mv[...]))
            totals.append(jnp.sum(scores, axis=1, keepdims=True))
            tops.append(highest)
        num_local[0] = per_head(sums)
        num_local[1] = per_head(totals) + jnp.zeros((rows, 128), F32)
        log_local[...] = per_head(tops) + jnp.zeros((rows, 128), F32)

    def scan_round(number):
        scan_copy(number).wait_recv()
        memory = st_in[number, 0:HEAD, :]
        ending = st_in[number, HEAD:HEAD + 8, :]

        @pl.when(sp >= lax.shift_left(jnp.int32(1), jnp.int32(number)))
        def _():
            done = joined((memory, ending), (st_before[0:HEAD, :], st_before[HEAD:HEAD + 8, :]))
            st_before[0:HEAD, :] = done[0]
            st_before[HEAD:HEAD + 8, :] = done[1]

        @pl.when(number < ROUNDS - 1)
        def _():
            mine = (st_out[number, 0:HEAD, :], st_out[number, HEAD:HEAD + 8, :])
            whole = joined((memory, ending), mine)
            reached = sp >= lax.shift_left(jnp.int32(1), jnp.int32(number))
            st_out[number + 1, 0:HEAD, :] = jnp.where(reached, whole[0], mine[0])
            st_out[number + 1, HEAD:HEAD + 8, :] = jnp.where(reached, whole[1], mine[1])

    def step_body(step, unused):
        def sub_step(number, unused):
            for stream in range(4):
                if stream % 2 == 0:
                    passing(stream, step - 1, number).wait_recv()

                    @pl.when(step < 16)
                    def _():
                        passing(stream, step - 1, number).wait_send()
                        passing(stream, step, number).start()
                else:
                    @pl.when(step < 16)
                    def _():
                        passing(stream, step - 1, number).wait_recv()

                    @pl.when(step < 15)
                    def _():
                        passing(stream, step - 1, number).wait_send()
                        passing(stream, step, number).start()
            if CHUNKS == 4:
                attend_stream(step - 1, number)
            else:
                for k in range(4 // CHUNKS):
                    attend_stream(step - 1, number * (4 // CHUNKS) + k)
            return unused

        lax.fori_loop(0, CHUNKS, sub_step, 0)

        @pl.when(step == 1)
        def _():
            local_memory()

        @pl.when((step % 3 == 2) & (step < 15))
        def _():
            scan_round(step // 3)

        @pl.when((step % 3 == 0) & (step < 13))
        def _():
            scan_copy(step // 3).start()

        return unused

    def attend_stream(step, stream):
        ring, way = stream // 2, stream % 2
        start = t0 + ring * (t1 - t0)
        position = (start + way * (2 * step) + SPANS - step) % SPANS
        first, second = span_on_ring(0, position), span_on_ring(1, position)
        origin = first + ring * (second - first)

        @pl.when(origin < sp)
        def _():
            visit(ring, position)

    lax.fori_loop(1, 17, step_body, 0)
    for number in range(CHUNKS):
        for stream in range(4):
            passing(stream, 15 if stream % 2 == 0 else 14, number).wait_send()
    attend_stream(16, 0)
    attend_stream(16, 2)
    for number in range(ROUNDS):
        scan_copy(number).wait_send()

    rooted = []
    for head in range(2):
        sides = []
        for side in range(2):
            part = acc[head, side * rows:(side + 1) * rows, :]
            sides.append(part / pltpu.roll(part, 64, 1))
        difference = sides[0] - lambdas[head] * sides[1]
        squared = jnp.where(low, 0.0, difference * difference)
        mean = jnp.sum(squared, axis=1, keepdims=True) * (1.0 / HEAD)
        rooted.append(difference * lax.rsqrt(mean + EPSILON))
    cat[:, 0:128] = (jnp.where(low, pltpu.roll(rooted[0], 64, 1), rooted[1])
                     * head_gain[...]).astype(BF16)

    start_memory = jnp.zeros((HEAD, 128), F32)
    start_tail = jnp.zeros((8, 128), F32)
    entered = joined((start_memory, start_tail), (st_before[0:HEAD, :], st_before[HEAD:HEAD + 8, :]))
    memory_in, normal_in, stable_in = entered[0], entered[1][0:1], entered[1][1:2]
    spread = jnp.concatenate(
        [jnp.where(low_square, memory_in, 0.0), jnp.where(low_square, 0.0, memory_in)], axis=0)
    spread_normal = jnp.concatenate(
        [jnp.where(low_square, normal_in, 0.0), jnp.where(low_square, 0.0, normal_in)], axis=0)
    carried_log = gates[0] + stable_in
    row_top = jnp.maximum(carried_log, log_local[...])
    outside = jnp.exp(carried_log - row_top)
    inside = jnp.exp(log_local[...] - row_top)
    high, small = halves(spread)
    numerator = outside * (dot_t(mq[...], high) + dot_t(mq[...], small)) + inside * num_local[0]
    high, small = halves(spread_normal)
    denominator = outside * (dot_t(mq[...], high) + dot_t(mq[...], small)) + inside * num_local[1]
    cat[:, 128:256] = (numerator / jnp.maximum(jnp.abs(denominator), 1.0)).astype(BF16)

    for load in out_loads:
        load.wait()
    both = cat[...]

    def share(seat):
        return dot(both, wo[seat]).astype(BF16)

    offsets = (2, 1, 3, 0)
    pairs = []
    for number, offset in enumerate(offsets):
        to_partner[number] = share(2 * ((y + offset) % 4) + 1 - c)
        pairs.append(remote(to_partner.at[number], from_partner.at[number], pair_send.at[number],
                            pair_recv.at[number], sp, partner))
        pairs[number].start()

    def summed(number):
        own = share(2 * ((y + offsets[number]) % 4) + c).astype(F32)
        pairs[number].wait_recv()
        return own + from_partner[number].astype(F32)

    def shift(number, seat):
        return remote(to_ring.at[number], from_ring.at[number], sum_send.at[number],
                      sum_recv.at[number], sp, seat)

    shifts = [shift(0, right), shift(1, left), shift(2, right), shift(3, right), shift(4, left),
              shift(5, left)]
    total = summed(0)
    to_ring[0] = total[:half_rows].astype(BF16)
    to_ring[1] = total[half_rows:].astype(BF16)
    shifts[0].start()
    shifts[1].start()
    total = summed(1)
    to_ring[2] = total[half_rows:].astype(BF16)
    shifts[2].start()
    rest = total[:half_rows]
    total = summed(2)
    to_ring[4] = total[:half_rows].astype(BF16)
    shifts[4].start()
    shifts[0].wait_recv()
    to_ring[3] = (rest + from_ring[0].astype(F32)).astype(BF16)
    shifts[3].start()
    shifts[1].wait_recv()
    to_ring[5] = (total[half_rows:] + from_ring[1].astype(F32)).astype(BF16)
    shifts[5].start()
    total = summed(3)
    for number in (2, 4):
        shifts[number].wait_recv()
    lower = total[half_rows:] + from_ring[2].astype(F32)
    upper = total[:half_rows] + from_ring[4].astype(F32)
    shifts[3].wait_recv()
    shifts[5].wait_recv()
    out[0:half_rows, :] = (upper + from_ring[3].astype(F32)).astype(BF16)
    out[half_rows:rows, :] = (lower + from_ring[5].astype(F32)).astype(BF16)
    for copy in pairs + shifts:
        copy.wait_send()


def per_device(
    inputs, norm_gain, query_weight, key_weight, value_weight, memory_query_weight,
    memory_key_weight, memory_value_weight, input_gate_weight, forget_gate_weight, forget_bias,
    decay_shift, lambdas, head_gain, out_weight_attention, out_weight_memory,
):
    rows, columns = inputs.shape
    positions = (lax.axis_index("sp") * rows + jnp.arange(rows, dtype=jnp.int32)).astype(F32)
    middle = DD // 2
    inverse = 1.0 / ROTARY_BASE ** (jnp.arange(middle, dtype=F32) / middle)
    angles = positions[:, None] * inverse[None, :]
    cosine, sine = jnp.cos(angles), jnp.sin(angles)
    cosine = jnp.concatenate([cosine] * 8, axis=1)
    sine = jnp.concatenate([-sine, sine] * 4, axis=1)
    vmem = pl.BlockSpec(memory_space=pltpu.VMEM)
    smem = pl.BlockSpec(memory_space=pltpu.SMEM)
    anywhere = pl.BlockSpec(memory_space=pl.ANY)
    half = rows // 2
    scratch = [
        pltpu.VMEM((8, rows, columns), BF16),
        pltpu.VMEM((8, rows, columns), BF16),
        pltpu.VMEM((rows, columns), F32),
        pltpu.VMEM((3, 2048, 256), BF16),
        pltpu.VMEM((2048, 2), BF16),
        pltpu.VMEM((2048, 2), BF16),
        pltpu.VMEM((8, 256, 256), BF16),
        pltpu.VMEM((2, SPANS, rows, 128), BF16),
        pltpu.VMEM((2, 2 * rows, 128), BF16),
        pltpu.VMEM((rows, 128), BF16),
        pltpu.VMEM((rows, 128), BF16),
        pltpu.VMEM((rows, 128), BF16),
        pltpu.VMEM((2, rows, 128), F32),
        pltpu.VMEM((2, 2 * rows, 128), F32),
        pltpu.VMEM((2, 2 * rows, 128), F32),
        pltpu.VMEM((ROUNDS, HEAD + 8, 128), F32),
        pltpu.VMEM((ROUNDS, HEAD + 8, 128), F32),
        pltpu.VMEM((HEAD + 8, 128), F32),
        pltpu.VMEM((2, rows, 128), F32),
        pltpu.VMEM((rows, 128), F32),
        pltpu.VMEM((rows, 256), BF16),
        pltpu.VMEM((4, rows, 256), BF16),
        pltpu.VMEM((4, rows, 256), BF16),
        pltpu.VMEM((6, half, 256), BF16),
        pltpu.VMEM((6, half, 256), BF16),
        pltpu.SemaphoreType.DMA((25,)),
        pltpu.SemaphoreType.DMA((13,)),
        pltpu.SemaphoreType.DMA((13,)),
        pltpu.SemaphoreType.DMA((4, CHUNKS)),
        pltpu.SemaphoreType.DMA((4, 16, CHUNKS)),
        pltpu.SemaphoreType.DMA((ROUNDS,)),
        pltpu.SemaphoreType.DMA((ROUNDS,)),
        pltpu.SemaphoreType.DMA((4,)),
        pltpu.SemaphoreType.DMA((4,)),
        pltpu.SemaphoreType.DMA((6,)),
        pltpu.SemaphoreType.DMA((6,)),
    ]
    return pl.pallas_call(
        layer_kernel,
        out_shape=jax.ShapeDtypeStruct((rows, columns), BF16),
        in_specs=[anywhere, vmem, vmem, vmem] + [anywhere] * 8
        + [smem, vmem, smem, vmem, anywhere, anywhere],
        out_specs=vmem,
        scratch_shapes=scratch,
        compiler_params=pltpu.CompilerParams(
            collective_id=0, has_side_effects=True, vmem_limit_bytes=60 * 1024 * 1024),
        name="layer",
    )(
        inputs, norm_gain.reshape(8, 1, 256), cosine, sine, query_weight, key_weight, value_weight,
        memory_query_weight, memory_key_weight, memory_value_weight, input_gate_weight,
        forget_gate_weight, forget_bias, decay_shift, lambdas,
        jnp.concatenate([head_gain, head_gain]).reshape(1, 128),
        out_weight_attention, out_weight_memory,
    )


def solution(mesh):
    split = P(None, "tp")
    placed = (
        P("sp", "tp"), P(), split, split, split, split, split, split, split, split,
        P("tp"), P("sp", "tp"), P("tp"), P(), P("tp", None), P("tp", None),
    )
    return jax.shard_map(
        per_device, mesh=mesh, in_specs=placed, out_specs=P("sp", "tp"), check_vma=False)
```

```python
import jax
import numpy as np
import jax.numpy as jnp
from jax import lax
from jax.experimental import pallas as pl
from jax.experimental.pallas import tpu as pltpu
from jax.sharding import PartitionSpec as P

HEAD = 64
DD = 32
EPSILON = 1e-06
ROTARY_BASE = 10000.0
NEGATIVE = -1e30
LOG2E = 1.4426950408889634
SPANS = 32
ROUNDS = 5
X_LAG = 2
RELAY_LAG = 1
MESH = pl.DeviceIdType.MESH
F32 = jnp.float32
BF16 = jnp.bfloat16


def dot(a, b):
    return jnp.dot(a, b, preferred_element_type=F32)


def dot_t(a, b):
    return lax.dot_general(a, b, (((1,), (1,)), ((), ())), preferred_element_type=F32)


def halves(a):
    high = a.astype(BF16)
    return high, (a - high.astype(F32)).astype(BF16)


def thirds(a):
    high = a.astype(BF16)
    rest = a - high.astype(F32)
    middle = rest.astype(BF16)
    return high, middle, (rest - middle.astype(F32)).astype(BF16)


def layer_kernel(
    x, gain, near_table, far_table, wq, wk, wv, wmq, wmk, wmv, wig, wfg, bias, decay, lambdas, head_gain,
    woa, wom, out,
    xg, xs, squares, w, wo, held, qs, mq, mk, mv, gates, gate_rows, acc, top, st_in, st_out, st_before,
    num_local, log_local, cat, to_partner, from_partner, to_ring, from_ring,
    load_sem, gather_send, gather_recv, z_send, z_recv, x_send, x_recv, scan_send, scan_recv,
    pair_send, pair_recv, sum_send, sum_recv,
):
    rows = x.shape[0]
    half_rows = rows // 2
    sp = lax.axis_index("sp")
    tp = lax.axis_index("tp")
    y, c = tp // 2, tp % 2
    right = 2 * ((y + 1) % 4) + c
    left = 2 * ((y + 3) % 4) + c
    across = 2 * ((y + 2) % 4) + c
    partner = 2 * y + 1 - c
    z, across_x = sp // 4, sp % 4
    above, below = 4 * ((z + 1) % 8) + across_x, 4 * ((z + 7) % 8) + across_x
    nexts = [above, below, 4 * z + (across_x + 1) % 4, 4 * z + (across_x + 3) % 4]

    def span_at(dz, dx):
        return 4 * ((z + dz + 16) % 8) + (across_x + dx) % 4

    def remote(src, dst, send, recv, span, seat):
        return pltpu.make_async_remote_copy(
            src_ref=src, dst_ref=dst, send_sem=send, recv_sem=recv,
            device_id=(span, seat), device_id_type=MESH)

    own_load = pltpu.make_async_copy(x, xg.at[tp], load_sem.at[0])
    own_load.start()
    loads = []
    for number, (weight, tile, at) in enumerate(
            ((wq, 0, 0), (wk, 0, 128), (wv, 1, 0), (wmq, 1, 128), (wmk, 2, 0), (wmv, 2, 128))):
        loads.append(pltpu.make_async_copy(
            weight, w.at[tile, :, pl.ds(at, 128)], load_sem.at[1 + number]))
    for load in loads:
        load.start()
    out_loads = []
    for j in range(8):
        for part, weight in enumerate((woa, wom)):
            out_loads.append(pltpu.make_async_copy(
                weight.at[:, pl.ds(256 * j, 256)], wo.at[j, pl.ds(128 * part, 128), :],
                load_sem.at[9 + 2 * j + part]))
    for load in out_loads:
        load.start()

    barrier = pltpu.get_barrier_semaphore()
    greeted = [(sp, right), (sp, left), (sp, partner)] + [(span, tp) for span in nexts]
    for number in range(ROUNDS):
        greeted.append(((sp + 2 ** number) % SPANS, tp))
        if number < ROUNDS - 1:
            greeted.append(((sp + SPANS - 2 ** number) % SPANS, tp))
    for span, seat in greeted:
        pl.semaphore_signal(barrier, inc=1, device_id=(span, seat), device_id_type=MESH)
    pl.semaphore_wait(barrier, len(greeted))

    def piece(seat, half):
        return xg.at[seat, pl.ds(half * half_rows, half_rows), :]

    def gather(number, ref, seat):
        return remote(ref, ref, gather_send.at[number], gather_recv.at[number], sp, seat)

    sends = {
        0: gather(0, piece(tp, 0), right),
        1: gather(1, piece(tp, 1), right),
        2: gather(2, piece(tp, 1), left),
        3: gather(3, piece(tp, 0), left),
        4: gather(4, xg.at[tp], partner),
        5: gather(5, piece(left, 0), right),
        6: gather(6, piece(left, 0), partner),
        7: gather(7, piece(right, 1), left),
        8: gather(8, piece(right, 1), partner),
        9: gather(9, piece(left, 1), partner),
        10: gather(10, piece(right, 0), partner),
        11: gather(11, piece(across, 0), partner),
        12: gather(12, piece(across, 1), partner),
    }
    own_load.wait()
    for number in (0, 2, 1, 3, 4):
        sends[number].start()

    def absorb(seat):
        block = xg[seat].astype(F32)
        squares[...] += block * block
        xs[seat] = (block * gain[seat]).astype(BF16)

    squares[...] = jnp.zeros_like(squares)
    absorb(tp)
    sends[0].wait_recv()
    sends[5].start()
    sends[6].start()
    sends[2].wait_recv()
    sends[7].start()
    sends[8].start()
    sends[4].wait_recv()
    absorb(partner)
    sends[1].wait_recv()
    sends[9].start()
    sends[3].wait_recv()
    sends[10].start()
    absorb(left)
    absorb(right)
    sends[5].wait_recv()
    sends[11].start()
    sends[7].wait_recv()
    sends[12].start()
    for number in (6, 8, 9, 10):
        sends[number].wait_recv()
    absorb(2 * ((y + 1) % 4) + 1 - c)
    absorb(2 * ((y + 3) % 4) + 1 - c)
    absorb(across)
    sends[11].wait_recv()
    sends[12].wait_recv()
    absorb(2 * ((y + 2) % 4) + 1 - c)
    for number in range(13):
        sends[number].wait_send()
    for load in loads:
        load.wait()

    inverse = lax.rsqrt(
        jnp.sum(squares[...], axis=1, keepdims=True) * (1.0 / 2048.0) + EPSILON)
    scaled = jnp.concatenate([xs[j] for j in range(8)], axis=1)
    lane = lax.broadcasted_iota(jnp.int32, (rows, 128), 1)
    low = lane < HEAD
    former = lane % 32 < 16

    far_cosine, far_sine = far_table[sp, 0:1, :], far_table[sp, 1:2, :]
    cosine = far_cosine * near_table[0] - far_sine * near_table[1]
    sine = far_sine * near_table[0] + far_cosine * near_table[1]
    sine = jnp.where(former, -sine, sine)

    def rotated(flat):
        floats = flat.astype(BF16).astype(F32)
        swapped = jnp.where(former, pltpu.roll(floats, 112, 1), pltpu.roll(floats, 16, 1))
        return (floats * cosine + swapped * sine).astype(BF16).astype(F32)

    product = dot(scaled, w[0]) * inverse
    queries = rotated(product[:, :128])
    keys = rotated(product[:, 128:])
    product = dot(scaled, w[1]) * inverse
    values = product[:, :128].astype(BF16).astype(F32)
    mq[...] = product[:, 128:].astype(BF16)
    held[0, sp] = jnp.where(low, keys, pltpu.roll(values, 64, 1)).astype(BF16)
    held[1, sp] = jnp.where(low, pltpu.roll(keys, 64, 1), values).astype(BF16)
    for head in range(2):
        turned = queries if head == 0 else pltpu.roll(queries, 64, 1)
        for side in range(2):
            inside = (lane >= DD * side) & (lane < DD * side + DD)
            qs[head, side * rows:(side + 1) * rows, :] = jnp.where(inside, turned, 0.0).astype(BF16)

    def z_copy(chain, way, hop, dx):
        dz = 1 - hop if way == 0 else hop - 1
        ref = held.at[1 if isinstance(chain, int) and chain == 0 else 0, span_at(dz, dx)]
        return remote(ref, ref, z_send.at[chain, way, hop - 1], z_recv.at[chain, way, hop - 1],
                      nexts[way], tp)

    def x_copy(number, kind, ring, dz):
        if kind < 2:
            ref = held.at[ring, span_at(dz, 0)]
        else:
            ref = held.at[ring, span_at(dz, 3 if kind == 2 else 1),
                          pl.ds((kind - 2) * half_rows, half_rows), :]
        return remote(ref, ref, x_send.at[number, kind], x_recv.at[number, kind],
                      nexts[2 + kind % 2], tp)

    for way in range(2):
        z_copy(0, way, 1, 0).start()
        x_copy(5, way, 0, 0).start()
    for way in range(2):
        z_copy(1, way, 1, 0).start()
        x_copy(0, way, 1, 0).start()

    product = dot(scaled, w[2]) * inverse
    mk[...] = product[:, :128].astype(BF16)
    mv[...] = product[:, 128:].astype(BF16)
    inverse_row = jnp.transpose(jnp.broadcast_to(inverse, (rows, 128)))[0:1, :]
    gate_in = dot_t(wig[...], scaled) * inverse_row
    forget = dot_t(wfg[...], scaled) * inverse_row

    def log_sigmoid(a):
        return jnp.minimum(a, 0.0) - jnp.log1p(jnp.exp(-jnp.abs(a)))

    def per_head(parts):
        return jnp.where(low, parts[0], parts[1])

    first_row = lax.broadcasted_iota(jnp.int32, (2, rows), 0) == 0
    log_forget = log_sigmoid(forget + jnp.where(first_row, bias[0], bias[1])) + decay[...]
    before_or_at = (lax.broadcasted_iota(jnp.int32, (rows, rows), 1)
                    <= lax.broadcasted_iota(jnp.int32, (rows, rows), 0))
    triangle = jnp.where(before_or_at, 1.0, 0.0).astype(BF16)
    high, middle, small = thirds(log_forget)
    cumulative = dot_t(high, triangle) + dot_t(middle, triangle) + dot_t(small, triangle)
    gate_rows[...] = gate_in - cumulative
    upper_rows = lax.broadcasted_iota(jnp.int32, (128, rows), 0) < HEAD

    def columns(pair):
        return jnp.transpose(jnp.where(upper_rows, pair[0:1, :], pair[1:2, :]))

    gates[0] = columns(cumulative)
    gates[1] = columns(gate_rows[...])
    span_decay = gates[0, rows - 1:rows, :]
    toward_end = span_decay + gates[1]
    span_top = jnp.max(toward_end, axis=0, keepdims=True)
    end_weights = jnp.exp(toward_end - span_top)
    key_floats = mk[...].astype(F32) * 0.125
    weighted = jnp.transpose(end_weights * mv[...].astype(F32))
    high, small = halves(weighted)
    keys_exact = key_floats.astype(BF16)
    outer = dot(high, keys_exact) + dot(small, keys_exact)
    row = lax.broadcasted_iota(jnp.int32, (8, 128), 0)

    def tail(normal, stable, decays):
        return jnp.where(row == 0, normal, jnp.where(row == 1, stable, decays))

    low_square = low[:HEAD]
    st_out[0, 0:HEAD, :] = jnp.where(low_square, outer[:HEAD], outer[HEAD:])
    st_out[0, HEAD:HEAD + 8, :] = tail(
        jnp.sum(end_weights * key_floats, axis=0, keepdims=True), span_top, span_decay)
    st_before[0:HEAD, :] = jnp.zeros((HEAD, 128), F32)
    st_before[HEAD:HEAD + 8, :] = tail(0.0, NEGATIVE, 0.0) + jnp.zeros((8, 128), F32)

    def scan_copy(number):
        target = (sp + lax.shift_left(jnp.int32(1), jnp.int32(number))) % SPANS
        return remote(st_out.at[number], st_in.at[number], scan_send.at[number],
                      scan_recv.at[number], target, tp)

    def joined(earlier, later):
        old, new = earlier[1], later[1]
        decays, stable, later_stable = new[2:3], old[1:2], new[1:2]
        highest = jnp.maximum(decays + stable, later_stable)
        first = jnp.exp(decays + stable - highest)
        second = jnp.exp(later_stable - highest)
        return (first * earlier[0] + second * later[0],
                tail(first * old[0:1] + second * new[0:1], highest, old[2:3] + decays))

    scale = DD ** (-0.5) * LOG2E
    ones_low = low

    def visit(ring, position, mask=None):
        block = held[ring, position]
        extended = jnp.where(ones_low, jnp.ones_like(block), block)
        scores = dot_t(qs[ring], block)
        if mask is not None:
            scores = jnp.where(mask, scores, NEGATIVE)
            highest = jnp.broadcast_to(jnp.max(scores, axis=1, keepdims=True), (2 * rows, 128))
        else:
            old = top[ring]
            highest = jnp.maximum(old, jnp.max(scores, axis=1, keepdims=True))
        shift = highest * scale
        weights = jnp.exp2(scores * scale - jnp.concatenate([shift] * (rows // 128), axis=1))
        product = dot(weights.astype(BF16), extended)
        if mask is not None:
            acc[ring] = product
        else:
            acc[ring] = acc[ring] * jnp.exp2((old - highest) * scale) + product
        top[ring] = highest

    causal = jnp.concatenate([before_or_at, before_or_at], axis=0)
    visit(0, sp, causal)
    scan_copy(0).start()
    x_copy(5, 0, 0, 0).wait_recv()
    x_copy(5, 2, 0, 0).start()
    for way in range(2):
        z_copy(2, way, 1, 3).start()
    x_copy(5, 1, 0, 0).wait_recv()
    x_copy(5, 3, 0, 0).start()
    for way in range(2):
        z_copy(3, way, 1, 1).start()
    visit(1, sp, causal)

    def local_memory():
        sums, tops, totals = [], [], []
        for head in range(2):
            inside = low if head == 0 else ~low
            gap = gates[0, :, HEAD * head:HEAD * head + 1] + gate_rows[head:head + 1, :]
            gap = jnp.where(before_or_at, gap, NEGATIVE)
            highest = jnp.max(gap, axis=1, keepdims=True)
            within = jnp.exp(gap - highest)
            mine = jnp.where(inside, mq[...].astype(F32), 0.0).astype(BF16)
            scores = within * (dot_t(mine, mk[...]) * 0.125)
            high, small = halves(scores)
            sums.append(dot(high, mv[...]) + dot(small, mv[...]))
            totals.append(jnp.sum(scores, axis=1, keepdims=True))
            tops.append(highest)
        num_local[0] = per_head(sums)
        num_local[1] = per_head(totals) + jnp.zeros((rows, 128), F32)
        log_local[...] = per_head(tops) + jnp.zeros((rows, 128), F32)

    def scan_round(number):
        scan_copy(number).wait_recv()
        memory = st_in[number, 0:HEAD, :]
        ending = st_in[number, HEAD:HEAD + 8, :]

        @pl.when(sp >= lax.shift_left(jnp.int32(1), jnp.int32(number)))
        def _():
            done = joined((memory, ending), (st_before[0:HEAD, :], st_before[HEAD:HEAD + 8, :]))
            st_before[0:HEAD, :] = done[0]
            st_before[HEAD:HEAD + 8, :] = done[1]

        @pl.when(number < ROUNDS - 1)
        def _():
            mine = (st_out[number, 0:HEAD, :], st_out[number, HEAD:HEAD + 8, :])
            whole = joined((memory, ending), mine)
            reached = sp >= lax.shift_left(jnp.int32(1), jnp.int32(number))
            st_out[number + 1, 0:HEAD, :] = jnp.where(reached, whole[0], mine[0])
            st_out[number + 1, HEAD:HEAD + 8, :] = jnp.where(reached, whole[1], mine[1])

    def attend(ring, dz, dx, valid):
        origin = span_at(dz, dx)

        @pl.when(valid & (origin < sp))
        def _():
            visit(ring, origin)

    def iteration(i, unused):
        pair, hop = i % 2, i // 2 + 1

        def by_way(ups, downs, then):
            def body(way, unused):
                pl.when(way == 0)(ups)
                pl.when(way == 1)(downs)
                then(way)
                return unused

            lax.fori_loop(0, 2, body, 0)

        def signed(way, distance):
            return (2 * way - 1) * distance

        @pl.when((i >= 1) & (i < ROUNDS))
        def _():
            scan_copy(i).start()

        def own_chain(way):
            last = 4 - way

            @pl.when(i < last)
            def _():
                z_copy(0, way, i + 1, 0).wait_recv()

                @pl.when(i < last - 1)
                def _():
                    z_copy(0, way, i + 2, 0).start()

                for kind in range(2):
                    x_copy(5 * way + i + 1, kind, 1, (2 * way - 1) * (i + 1)).start()

        by_way(lambda: own_chain(0), lambda: own_chain(1),
               lambda way: attend(1, signed(way, i + 1), 0, i < 4 - way))

        def x_arrival(rows_way, kind):
            valid = (i <= 4) if rows_way == 0 else (i >= 1) & (i <= 3)

            @pl.when(valid)
            def _():
                dz = (2 * rows_way - 1) * i
                x_copy(5 * rows_way + i, kind, 1, dz).wait_recv()
                x_copy(5 * rows_way + i, kind + 2, 1, dz).start()

        def x_attend(rows_way, side):
            j = i - X_LAG
            valid = (j >= 0) & (j <= 4) if rows_way == 0 else (j >= 1) & (j <= 3)
            attend(1, (2 * rows_way - 1) * j, 3 - 2 * side, valid)

        by_way(lambda: x_arrival(0, 0), lambda: x_arrival(0, 1), lambda side: x_attend(0, side))

        @pl.when(i == 0)
        def _():
            x_copy(5, 2, 0, 0).wait_recv()
            x_copy(5, 3, 0, 0).wait_recv()
            for way in range(2):
                z_copy(4, way, 1, 2).start()

        def chain(number, way, dx, last):
            @pl.when(hop <= last)
            def _():
                z_copy(number, way, hop, dx).wait_recv()

                @pl.when(hop < last)
                def _():
                    z_copy(number, way, hop + 1, dx).start()

        first = 1 + 2 * pair
        by_way(lambda: chain(first, 0, pair, 4), lambda: chain(first, 1, pair, 3),
               lambda way: attend(0, signed(way, hop), pair, hop <= 4 - way))
        by_way(lambda: x_arrival(1, 0), lambda: x_arrival(1, 1), lambda side: x_attend(1, side))
        by_way(lambda: chain(first + 1, 0, 3 - pair, 3), lambda: chain(first + 1, 1, 3 - pair, 4),
               lambda way: attend(0, signed(way, hop), 3 - pair, hop <= 3 + way))

        def relayed(rows_way):
            j = i - 1
            valid = (j >= 0) & (j <= 4) if rows_way == 0 else (j >= 1) & (j <= 3)

            @pl.when(valid)
            def _():
                for kind in (2, 3):
                    x_copy(5 * rows_way + j, kind, 1, (2 * rows_way - 1) * j).wait_recv()

        def relay_attend(way):
            j = i - 1 - RELAY_LAG
            own = way == 2
            valid = jnp.where(own, i < 3, (j >= way) & (j <= 4 - way))
            attend(jnp.where(own, 0, 1), jnp.where(own, 0, signed(way, j)),
                   jnp.where(own, 3 - i, 2), valid)

        def body(way, unused):
            pl.when(way == 0)(lambda: relayed(0))
            pl.when(way == 1)(lambda: relayed(1))
            relay_attend(way)
            return unused

        lax.fori_loop(0, 3, body, 0)

        @pl.when(i == 0)
        def _():
            local_memory()

        @pl.when(i < ROUNDS)
        def _():
            scan_round(i)

        return unused

    lax.fori_loop(0, 8, iteration, 0)
    for number in range(5):
        for way in range(2):
            last = 4 if (number in (2, 4)) == (way == 1) else 3
            for hop in range(1, last + 1):
                z_copy(number, way, hop, 0).wait_send()
    for number in (0, 1, 2, 3, 4, 5, 6, 7, 8):
        for kind in range(4):
            x_copy(number, kind, 1, 0).wait_send()
    for number in range(ROUNDS):
        scan_copy(number).wait_send()

    rooted = []
    for head in range(2):
        sides = []
        for side in range(2):
            part = acc[head, side * rows:(side + 1) * rows, :]
            sides.append(part / pltpu.roll(part, 64, 1))
        difference = sides[0] - lambdas[head] * sides[1]
        squared = jnp.where(low, 0.0, difference * difference)
        mean = jnp.sum(squared, axis=1, keepdims=True) * (1.0 / HEAD)
        rooted.append(difference * lax.rsqrt(mean + EPSILON))
    cat[:, 0:128] = (jnp.where(low, pltpu.roll(rooted[0], 64, 1), rooted[1])
                     * jnp.concatenate([head_gain[...]] * 2, axis=1)).astype(BF16)

    start_memory = jnp.zeros((HEAD, 128), F32)
    start_tail = jnp.zeros((8, 128), F32)
    entered = joined((start_memory, start_tail), (st_before[0:HEAD, :], st_before[HEAD:HEAD + 8, :]))
    memory_in, normal_in, stable_in = entered[0], entered[1][0:1], entered[1][1:2]
    spread = jnp.concatenate(
        [jnp.where(low_square, memory_in, 0.0), jnp.where(low_square, 0.0, memory_in)], axis=0)
    spread_normal = jnp.concatenate(
        [jnp.where(low_square, normal_in, 0.0), jnp.where(low_square, 0.0, normal_in)], axis=0)
    carried_log = gates[0] + stable_in
    row_top = jnp.maximum(carried_log, log_local[...])
    outside = jnp.exp(carried_log - row_top)
    inside = jnp.exp(log_local[...] - row_top)
    high, small = halves(spread)
    numerator = outside * (dot_t(mq[...], high) + dot_t(mq[...], small)) + inside * num_local[0]
    high, small = halves(spread_normal)
    denominator = outside * (dot_t(mq[...], high) + dot_t(mq[...], small)) + inside * num_local[1]
    cat[:, 128:256] = (numerator / jnp.maximum(jnp.abs(denominator), 1.0)).astype(BF16)

    for load in out_loads:
        load.wait()
    both = cat[...]

    def share(seat):
        return dot(both, wo[seat]).astype(BF16)

    offsets = (2, 1, 3, 0)
    pairs = []
    for number, offset in enumerate(offsets):
        to_partner[number] = share(2 * ((y + offset) % 4) + 1 - c)
        pairs.append(remote(to_partner.at[number], from_partner.at[number], pair_send.at[number],
                            pair_recv.at[number], sp, partner))
        pairs[number].start()

    def summed(number):
        own = share(2 * ((y + offsets[number]) % 4) + c).astype(F32)
        pairs[number].wait_recv()
        return own + from_partner[number].astype(F32)

    def shift(number, seat):
        return remote(to_ring.at[number], from_ring.at[number], sum_send.at[number],
                      sum_recv.at[number], sp, seat)

    shifts = [shift(0, right), shift(1, left), shift(2, right), shift(3, right), shift(4, left),
              shift(5, left)]
    total = summed(0)
    to_ring[0] = total[:half_rows].astype(BF16)
    to_ring[1] = total[half_rows:].astype(BF16)
    shifts[0].start()
    shifts[1].start()
    total = summed(1)
    to_ring[2] = total[half_rows:].astype(BF16)
    shifts[2].start()
    rest = total[:half_rows]
    total = summed(2)
    to_ring[4] = total[:half_rows].astype(BF16)
    shifts[4].start()
    shifts[0].wait_recv()
    to_ring[3] = (rest + from_ring[0].astype(F32)).astype(BF16)
    shifts[3].start()
    shifts[1].wait_recv()
    to_ring[5] = (total[half_rows:] + from_ring[1].astype(F32)).astype(BF16)
    shifts[5].start()
    total = summed(3)
    for number in (2, 4):
        shifts[number].wait_recv()
    lower = total[half_rows:] + from_ring[2].astype(F32)
    upper = total[:half_rows] + from_ring[4].astype(F32)
    shifts[3].wait_recv()
    shifts[5].wait_recv()
    out[0:half_rows, :] = (upper + from_ring[3].astype(F32)).astype(BF16)
    out[half_rows:rows, :] = (lower + from_ring[5].astype(F32)).astype(BF16)
    for copy in pairs + shifts:
        copy.wait_send()


def per_device(
    inputs, norm_gain, query_weight, key_weight, value_weight, memory_query_weight,
    memory_key_weight, memory_value_weight, input_gate_weight, forget_gate_weight, forget_bias,
    decay_shift, lambdas, head_gain, out_weight_attention, out_weight_memory,
):
    rows, columns = inputs.shape
    middle = DD // 2
    inverse = 1.0 / ROTARY_BASE ** (np.arange(middle) / middle)
    near = np.tile(np.arange(rows)[:, None] * inverse[None, :], (1, 8))
    far = np.tile((np.arange(SPANS) * rows)[:, None] * inverse[None, :], (1, 8))
    near = jnp.asarray(np.stack([np.cos(near), np.sin(near)]), F32)
    far = jnp.asarray(np.stack([np.cos(far), np.sin(far)], axis=1), F32)
    vmem = pl.BlockSpec(memory_space=pltpu.VMEM)
    smem = pl.BlockSpec(memory_space=pltpu.SMEM)
    anywhere = pl.BlockSpec(memory_space=pl.ANY)
    half = rows // 2
    scratch = [
        pltpu.VMEM((8, rows, columns), BF16),
        pltpu.VMEM((8, rows, columns), BF16),
        pltpu.VMEM((rows, columns), F32),
        pltpu.VMEM((3, 2048, 256), BF16),
        pltpu.VMEM((8, 256, 256), BF16),
        pltpu.VMEM((2, SPANS, rows, 128), BF16),
        pltpu.VMEM((2, 2 * rows, 128), BF16),
        pltpu.VMEM((rows, 128), BF16),
        pltpu.VMEM((rows, 128), BF16),
        pltpu.VMEM((rows, 128), BF16),
        pltpu.VMEM((2, rows, 128), F32),
        pltpu.VMEM((2, rows), F32),
        pltpu.VMEM((2, 2 * rows, 128), F32),
        pltpu.VMEM((2, 2 * rows, 128), F32),
        pltpu.VMEM((ROUNDS, HEAD + 8, 128), F32),
        pltpu.VMEM((ROUNDS, HEAD + 8, 128), F32),
        pltpu.VMEM((HEAD + 8, 128), F32),
        pltpu.VMEM((2, rows, 128), F32),
        pltpu.VMEM((rows, 128), F32),
        pltpu.VMEM((rows, 256), BF16),
        pltpu.VMEM((4, rows, 256), BF16),
        pltpu.VMEM((4, rows, 256), BF16),
        pltpu.VMEM((6, half, 256), BF16),
        pltpu.VMEM((6, half, 256), BF16),
        pltpu.SemaphoreType.DMA((25,)),
        pltpu.SemaphoreType.DMA((13,)),
        pltpu.SemaphoreType.DMA((13,)),
        pltpu.SemaphoreType.DMA((5, 2, 4)),
        pltpu.SemaphoreType.DMA((5, 2, 4)),
        pltpu.SemaphoreType.DMA((10, 4)),
        pltpu.SemaphoreType.DMA((10, 4)),
        pltpu.SemaphoreType.DMA((ROUNDS,)),
        pltpu.SemaphoreType.DMA((ROUNDS,)),
        pltpu.SemaphoreType.DMA((4,)),
        pltpu.SemaphoreType.DMA((4,)),
        pltpu.SemaphoreType.DMA((6,)),
        pltpu.SemaphoreType.DMA((6,)),
    ]
    return pl.pallas_call(
        layer_kernel,
        out_shape=jax.ShapeDtypeStruct((rows, columns), BF16),
        in_specs=[anywhere, vmem, vmem, vmem] + [anywhere] * 6 + [vmem, vmem]
        + [smem, vmem, smem, vmem, anywhere, anywhere],
        out_specs=vmem,
        scratch_shapes=scratch,
        compiler_params=pltpu.CompilerParams(
            collective_id=0, has_side_effects=True, vmem_limit_bytes=60 * 1024 * 1024),
        name="layer",
    )(
        inputs, norm_gain.reshape(8, 1, 256), near, far, query_weight, key_weight, value_weight,
        memory_query_weight, memory_key_weight, memory_value_weight, input_gate_weight.T,
        forget_gate_weight.T, forget_bias, decay_shift.T, lambdas, head_gain.reshape(1, HEAD),
        out_weight_attention, out_weight_memory,
    )


def solution(mesh):
    split = P(None, "tp")
    placed = (
        P("sp", "tp"), P(), split, split, split, split, split, split, split, split,
        P("tp"), P("sp", "tp"), P("tp"), P(), P("tp", None), P("tp", None),
    )
    return jax.shard_map(
        per_device, mesh=mesh, in_specs=placed, out_specs=P("sp", "tp"), check_vma=False)
```

```python
import jax
import numpy as np
import jax.numpy as jnp
from jax import lax
from jax.experimental import pallas as pl
from jax.experimental.pallas import tpu as pltpu
from jax.sharding import PartitionSpec as P

HEAD = 64
DD = 32
EPSILON = 1e-06
ROTARY_BASE = 10000.0
NEGATIVE = -1e30
LOG2E = 1.4426950408889634
SPANS = 32
ROUNDS = 5
X_LAG = 2
RELAY_LAG = 1
MESH = pl.DeviceIdType.MESH
F32 = jnp.float32
BF16 = jnp.bfloat16


def dot(a, b):
    return jnp.dot(a, b, preferred_element_type=F32)


def dot_t(a, b):
    return lax.dot_general(a, b, (((1,), (1,)), ((), ())), preferred_element_type=F32)


def halves(a):
    high = a.astype(BF16)
    return high, (a - high.astype(F32)).astype(BF16)


def thirds(a):
    high = a.astype(BF16)
    rest = a - high.astype(F32)
    middle = rest.astype(BF16)
    return high, middle, (rest - middle.astype(F32)).astype(BF16)


def layer_kernel(
    x, gain_in, near_in, far_in, wq, wk, wv, wmq, wmk, wmv, wig_in, wfg_in, bias_in, decay_in,
    lambdas_in, head_gain_in, woa, wom, out,
    gain, near_table, far_table, wig, wfg, bias, decay, lambdas, head_gain,
    xg, xs, squares, w, wo, held, qs, mq, mk, mv, gates, gate_rows, acc, top, st_in, st_out, st_before,
    num_local, log_local, cat, to_partner, from_partner, to_ring, from_ring,
    small_sem, load_sem, gather_send, gather_recv, z_send, z_recv, x_send, x_recv, scan_send, scan_recv,
    pair_send, pair_recv, sum_send, sum_recv,
):
    rows = x.shape[0]
    half_rows = rows // 2
    sp = lax.axis_index("sp")
    tp = lax.axis_index("tp")
    y, c = tp // 2, tp % 2
    right = 2 * ((y + 1) % 4) + c
    left = 2 * ((y + 3) % 4) + c
    across = 2 * ((y + 2) % 4) + c
    partner = 2 * y + 1 - c
    z, across_x = sp // 4, sp % 4
    above, below = 4 * ((z + 1) % 8) + across_x, 4 * ((z + 7) % 8) + across_x
    nexts = [above, below, 4 * z + (across_x + 1) % 4, 4 * z + (across_x + 3) % 4]

    def span_at(dz, dx):
        return 4 * ((z + dz + 16) % 8) + (across_x + dx) % 4

    def remote(src, dst, send, recv, span, seat):
        return pltpu.make_async_remote_copy(
            src_ref=src, dst_ref=dst, send_sem=send, recv_sem=recv,
            device_id=(span, seat), device_id_type=MESH)

    barrier = pltpu.get_barrier_semaphore()
    greeted = [(sp, right), (sp, left), (sp, partner)] + [(span, tp) for span in nexts]
    for number in range(ROUNDS):
        greeted.append(((sp + 2 ** number) % SPANS, tp))
        if number < ROUNDS - 1:
            greeted.append(((sp + SPANS - 2 ** number) % SPANS, tp))
    for span, seat in greeted:
        pl.semaphore_signal(barrier, inc=1, device_id=(span, seat), device_id_type=MESH)

    own_load = pltpu.make_async_copy(x, xg.at[tp], load_sem.at[0])
    own_load.start()
    loads = []
    for number, (weight, tile, at) in enumerate(
            ((wq, 0, 0), (wk, 0, 128), (wv, 1, 0), (wmq, 1, 128), (wmk, 2, 0), (wmv, 2, 128))):
        loads.append(pltpu.make_async_copy(
            weight, w.at[tile, :, pl.ds(at, 128)], load_sem.at[1 + number]))
    small_loads = {}
    for number, (source, target) in enumerate((
            (gain_in, gain), (near_in, near_table), (far_in.at[sp], far_table), (wig_in, wig),
            (wfg_in, wfg), (bias_in, bias), (decay_in, decay), (lambdas_in, lambdas),
            (head_gain_in, head_gain))):
        small_loads[number] = pltpu.make_async_copy(source, target, small_sem.at[number])
        small_loads[number].start()
    for load in loads:
        load.start()
    out_loads = []
    for j in range(8):
        for part, weight in enumerate((woa, wom)):
            out_loads.append(pltpu.make_async_copy(
                weight.at[:, pl.ds(256 * j, 256)], wo.at[j, pl.ds(128 * part, 128), :],
                load_sem.at[9 + 2 * j + part]))
    for load in out_loads:
        load.start()

    pl.semaphore_wait(barrier, len(greeted))

    def piece(seat, half):
        return xg.at[seat, pl.ds(half * half_rows, half_rows), :]

    def gather(number, ref, seat):
        return remote(ref, ref, gather_send.at[number], gather_recv.at[number], sp, seat)

    sends = {
        0: gather(0, piece(tp, 0), right),
        1: gather(1, piece(tp, 1), right),
        2: gather(2, piece(tp, 1), left),
        3: gather(3, piece(tp, 0), left),
        4: gather(4, xg.at[tp], partner),
        5: gather(5, piece(left, 0), right),
        6: gather(6, piece(left, 0), partner),
        7: gather(7, piece(right, 1), left),
        8: gather(8, piece(right, 1), partner),
        9: gather(9, piece(left, 1), partner),
        10: gather(10, piece(right, 0), partner),
        11: gather(11, piece(across, 0), partner),
        12: gather(12, piece(across, 1), partner),
    }
    own_load.wait()
    for number in (0, 2, 1, 3, 4):
        sends[number].start()

    def absorb(seat):
        block = xg[seat].astype(F32)
        squares[...] += block * block
        xs[seat] = (block * gain[seat]).astype(BF16)

    squares[...] = jnp.zeros_like(squares)
    small_loads[0].wait()
    absorb(tp)
    sends[0].wait_recv()
    sends[5].start()
    sends[6].start()
    sends[2].wait_recv()
    sends[7].start()
    sends[8].start()
    sends[4].wait_recv()
    absorb(partner)
    sends[1].wait_recv()
    sends[9].start()
    sends[3].wait_recv()
    sends[10].start()
    absorb(left)
    absorb(right)
    sends[5].wait_recv()
    sends[11].start()
    sends[7].wait_recv()
    sends[12].start()
    for number in (6, 8, 9, 10):
        sends[number].wait_recv()
    absorb(2 * ((y + 1) % 4) + 1 - c)
    absorb(2 * ((y + 3) % 4) + 1 - c)
    absorb(across)
    sends[11].wait_recv()
    sends[12].wait_recv()
    absorb(2 * ((y + 2) % 4) + 1 - c)
    for number in range(13):
        sends[number].wait_send()
    for load in loads + [small_loads[number] for number in range(1, 9)]:
        load.wait()

    inverse = lax.rsqrt(
        jnp.sum(squares[...], axis=1, keepdims=True) * (1.0 / 2048.0) + EPSILON)
    scaled = jnp.concatenate([xs[j] for j in range(8)], axis=1)
    lane = lax.broadcasted_iota(jnp.int32, (rows, 128), 1)
    low = lane < HEAD
    former = lane % 32 < 16

    far_cosine, far_sine = far_table[0:1, :], far_table[1:2, :]
    cosine = far_cosine * near_table[0] - far_sine * near_table[1]
    sine = far_sine * near_table[0] + far_cosine * near_table[1]
    sine = jnp.where(former, -sine, sine)

    def rotated(flat):
        floats = flat.astype(BF16).astype(F32)
        swapped = jnp.where(former, pltpu.roll(floats, 112, 1), pltpu.roll(floats, 16, 1))
        return (floats * cosine + swapped * sine).astype(BF16).astype(F32)

    product = dot(scaled, w[0]) * inverse
    queries = rotated(product[:, :128])
    keys = rotated(product[:, 128:])
    product = dot(scaled, w[1]) * inverse
    values = product[:, :128].astype(BF16).astype(F32)
    mq[...] = product[:, 128:].astype(BF16)
    held[0, sp] = jnp.where(low, keys, pltpu.roll(values, 64, 1)).astype(BF16)
    held[1, sp] = jnp.where(low, pltpu.roll(keys, 64, 1), values).astype(BF16)
    def z_copy(chain, way, hop, dx):
        dz = 1 - hop if way == 0 else hop - 1
        ref = held.at[1 if isinstance(chain, int) and chain == 0 else 0, span_at(dz, dx)]
        return remote(ref, ref, z_send.at[chain, way, hop - 1], z_recv.at[chain, way, hop - 1],
                      nexts[way], tp)

    def x_copy(number, kind, ring, dz):
        if kind < 2:
            ref = held.at[ring, span_at(dz, 0)]
        else:
            ref = held.at[ring, span_at(dz, 3 if kind == 2 else 1),
                          pl.ds((kind - 2) * half_rows, half_rows), :]
        return remote(ref, ref, x_send.at[number, kind], x_recv.at[number, kind],
                      nexts[2 + kind % 2], tp)

    for way in range(2):
        z_copy(0, way, 1, 0).start()
        x_copy(5, way, 0, 0).start()
    for way in range(2):
        z_copy(1, way, 1, 0).start()
        x_copy(0, way, 1, 0).start()

    for head in range(2):
        turned = queries if head == 0 else pltpu.roll(queries, 64, 1)
        for side in range(2):
            inside = (lane >= DD * side) & (lane < DD * side + DD)
            qs[head, side * rows:(side + 1) * rows, :] = jnp.where(inside, turned, 0.0).astype(BF16)
    product = dot(scaled, w[2]) * inverse
    mk[...] = product[:, :128].astype(BF16)
    mv[...] = product[:, 128:].astype(BF16)
    inverse_row = jnp.transpose(jnp.broadcast_to(inverse, (rows, 128)))[0:1, :]
    gate_in = dot_t(wig[...], scaled) * inverse_row
    forget = dot_t(wfg[...], scaled) * inverse_row

    def log_sigmoid(a):
        return jnp.minimum(a, 0.0) - jnp.log1p(jnp.exp(-jnp.abs(a)))

    def per_head(parts):
        return jnp.where(low, parts[0], parts[1])

    first_row = lax.broadcasted_iota(jnp.int32, (2, rows), 0) == 0
    log_forget = log_sigmoid(forget + jnp.where(first_row, bias[0], bias[1])) + decay[...]
    before_or_at = (lax.broadcasted_iota(jnp.int32, (rows, rows), 1)
                    <= lax.broadcasted_iota(jnp.int32, (rows, rows), 0))
    triangle = jnp.where(before_or_at, 1.0, 0.0).astype(BF16)
    high, middle, small = thirds(log_forget)
    cumulative = dot_t(high, triangle) + dot_t(middle, triangle) + dot_t(small, triangle)
    gate_rows[...] = gate_in - cumulative
    upper_rows = lax.broadcasted_iota(jnp.int32, (128, rows), 0) < HEAD

    def columns(pair):
        return jnp.transpose(jnp.where(upper_rows, pair[0:1, :], pair[1:2, :]))

    gates[0] = columns(cumulative)
    gates[1] = columns(gate_rows[...])
    span_decay = gates[0, rows - 1:rows, :]
    toward_end = span_decay + gates[1]
    span_top = jnp.max(toward_end, axis=0, keepdims=True)
    end_weights = jnp.exp(toward_end - span_top)
    key_floats = mk[...].astype(F32) * 0.125
    weighted = jnp.transpose(end_weights * mv[...].astype(F32))
    high, small = halves(weighted)
    keys_exact = key_floats.astype(BF16)
    outer = dot(high, keys_exact) + dot(small, keys_exact)
    row = lax.broadcasted_iota(jnp.int32, (8, 128), 0)

    def tail(normal, stable, decays):
        return jnp.where(row == 0, normal, jnp.where(row == 1, stable, decays))

    low_square = low[:HEAD]
    st_out[0, 0:HEAD, :] = jnp.where(low_square, outer[:HEAD], outer[HEAD:])
    st_out[0, HEAD:HEAD + 8, :] = tail(
        jnp.sum(end_weights * key_floats, axis=0, keepdims=True), span_top, span_decay)
    st_before[0:HEAD, :] = jnp.zeros((HEAD, 128), F32)
    st_before[HEAD:HEAD + 8, :] = tail(0.0, NEGATIVE, 0.0) + jnp.zeros((8, 128), F32)

    def scan_copy(number):
        target = (sp + lax.shift_left(jnp.int32(1), jnp.int32(number))) % SPANS
        return remote(st_out.at[number], st_in.at[number], scan_send.at[number],
                      scan_recv.at[number], target, tp)

    def joined(earlier, later):
        old, new = earlier[1], later[1]
        decays, stable, later_stable = new[2:3], old[1:2], new[1:2]
        highest = jnp.maximum(decays + stable, later_stable)
        first = jnp.exp(decays + stable - highest)
        second = jnp.exp(later_stable - highest)
        return (first * earlier[0] + second * later[0],
                tail(first * old[0:1] + second * new[0:1], highest, old[2:3] + decays))

    scale = DD ** (-0.5) * LOG2E
    ones_low = low

    def visit(ring, position, mask=None):
        block = held[ring, position]
        extended = jnp.where(ones_low, jnp.ones_like(block), block)
        scores = dot_t(qs[ring], block)
        if mask is not None:
            scores = jnp.where(mask, scores, NEGATIVE)
            highest = jnp.broadcast_to(jnp.max(scores, axis=1, keepdims=True), (2 * rows, 128))
        else:
            old = top[ring]
            highest = jnp.maximum(old, jnp.max(scores, axis=1, keepdims=True))
        shift = highest * scale
        weights = jnp.exp2(scores * scale - jnp.concatenate([shift] * (rows // 128), axis=1))
        product = dot(weights.astype(BF16), extended)
        if mask is not None:
            acc[ring] = product
        else:
            acc[ring] = acc[ring] * jnp.exp2((old - highest) * scale) + product
        top[ring] = highest

    causal = jnp.concatenate([before_or_at, before_or_at], axis=0)
    visit(0, sp, causal)
    scan_copy(0).start()
    x_copy(5, 0, 0, 0).wait_recv()
    x_copy(5, 2, 0, 0).start()
    for way in range(2):
        z_copy(2, way, 1, 3).start()
    x_copy(5, 1, 0, 0).wait_recv()
    x_copy(5, 3, 0, 0).start()
    for way in range(2):
        z_copy(3, way, 1, 1).start()
    visit(1, sp, causal)

    def local_memory():
        sums, tops, totals = [], [], []
        for head in range(2):
            inside = low if head == 0 else ~low
            gap = gates[0, :, HEAD * head:HEAD * head + 1] + gate_rows[head:head + 1, :]
            gap = jnp.where(before_or_at, gap, NEGATIVE)
            highest = jnp.max(gap, axis=1, keepdims=True)
            within = jnp.exp(gap - highest)
            mine = jnp.where(inside, mq[...].astype(F32), 0.0).astype(BF16)
            scores = within * (dot_t(mine, mk[...]) * 0.125)
            high, small = halves(scores)
            sums.append(dot(high, mv[...]) + dot(small, mv[...]))
            totals.append(jnp.sum(scores, axis=1, keepdims=True))
            tops.append(highest)
        num_local[0] = per_head(sums)
        num_local[1] = per_head(totals) + jnp.zeros((rows, 128), F32)
        log_local[...] = per_head(tops) + jnp.zeros((rows, 128), F32)

    def scan_round(number):
        scan_copy(number).wait_recv()
        memory = st_in[number, 0:HEAD, :]
        ending = st_in[number, HEAD:HEAD + 8, :]

        @pl.when(sp >= lax.shift_left(jnp.int32(1), jnp.int32(number)))
        def _():
            done = joined((memory, ending), (st_before[0:HEAD, :], st_before[HEAD:HEAD + 8, :]))
            st_before[0:HEAD, :] = done[0]
            st_before[HEAD:HEAD + 8, :] = done[1]

        @pl.when(number < ROUNDS - 1)
        def _():
            mine = (st_out[number, 0:HEAD, :], st_out[number, HEAD:HEAD + 8, :])
            whole = joined((memory, ending), mine)
            reached = sp >= lax.shift_left(jnp.int32(1), jnp.int32(number))
            st_out[number + 1, 0:HEAD, :] = jnp.where(reached, whole[0], mine[0])
            st_out[number + 1, HEAD:HEAD + 8, :] = jnp.where(reached, whole[1], mine[1])

    def attend(ring, dz, dx, valid):
        origin = span_at(dz, dx)

        @pl.when(valid & (origin < sp))
        def _():
            visit(ring, origin)

    def iteration(i, unused):
        pair, hop = i % 2, i // 2 + 1

        def by_way(ups, downs, then):
            def body(way, unused):
                pl.when(way == 0)(ups)
                pl.when(way == 1)(downs)
                then(way)
                return unused

            lax.fori_loop(0, 2, body, 0)

        def signed(way, distance):
            return (2 * way - 1) * distance

        @pl.when((i >= 1) & (i < ROUNDS))
        def _():
            scan_copy(i).start()

        def own_chain(way):
            last = 4 - way

            @pl.when(i < last)
            def _():
                z_copy(0, way, i + 1, 0).wait_recv()

                @pl.when(i < last - 1)
                def _():
                    z_copy(0, way, i + 2, 0).start()

                for kind in range(2):
                    x_copy(5 * way + i + 1, kind, 1, (2 * way - 1) * (i + 1)).start()

        by_way(lambda: own_chain(0), lambda: own_chain(1),
               lambda way: attend(1, signed(way, i + 1), 0, i < 4 - way))

        def x_arrival(rows_way, kind):
            valid = (i <= 4) if rows_way == 0 else (i >= 1) & (i <= 3)

            @pl.when(valid)
            def _():
                dz = (2 * rows_way - 1) * i
                x_copy(5 * rows_way + i, kind, 1, dz).wait_recv()
                x_copy(5 * rows_way + i, kind + 2, 1, dz).start()

        def x_attend(rows_way, side):
            j = i - X_LAG
            valid = (j >= 0) & (j <= 4) if rows_way == 0 else (j >= 1) & (j <= 3)
            attend(1, (2 * rows_way - 1) * j, 3 - 2 * side, valid)

        by_way(lambda: x_arrival(0, 0), lambda: x_arrival(0, 1), lambda side: x_attend(0, side))

        @pl.when(i == 0)
        def _():
            x_copy(5, 2, 0, 0).wait_recv()
            x_copy(5, 3, 0, 0).wait_recv()
            z_copy(4, 0, 1, 2).start()

        def chain(number, way, dx, last):
            @pl.when(hop <= last)
            def _():
                z_copy(number, way, hop, dx).wait_recv()

                @pl.when(hop < last)
                def _():
                    z_copy(number, way, hop + 1, dx).start()

        first = 1 + 2 * pair

        def first_downwards():
            chain(first, 1, pair, 4)

            @pl.when(pair == 1)
            def _():
                x_copy(9 + hop, 3, 0, hop).start()

        def second_downwards():
            @pl.when(pair == 0)
            def _():
                chain(2, 1, 3, 4)
                x_copy(9 + hop, 2, 0, hop).start()

            @pl.when((pair == 1) & (hop >= 2))
            def _():
                for kind in (2, 3):
                    x_copy(8 + hop, kind, 0, hop - 1).wait_recv()

        by_way(lambda: chain(first, 0, pair, 3), first_downwards,
               lambda way: attend(0, signed(way, hop), pair, hop <= 3 + way))
        by_way(lambda: x_arrival(1, 0), lambda: x_arrival(1, 1), lambda side: x_attend(1, side))
        by_way(lambda: chain(first + 1, 0, 3 - pair, 3), second_downwards,
               lambda way: attend(0, signed(way, hop - pair * way), 3 - pair,
                                  (hop >= 1 + pair * way) & (hop <= 3 + way)))

        def relayed(rows_way):
            j = i - 1
            valid = (j >= 0) & (j <= 4) if rows_way == 0 else (j >= 1) & (j <= 3)

            @pl.when(valid)
            def _():
                for kind in (2, 3):
                    x_copy(5 * rows_way + j, kind, 1, (2 * rows_way - 1) * j).wait_recv()

        def relay_attend(way):
            j = i - 1 - RELAY_LAG
            own = way == 2
            valid = jnp.where(own, i < 3, (j >= way) & (j <= 4 - way))
            attend(jnp.where(own, 0, 1), jnp.where(own, 0, signed(way, j)),
                   jnp.where(own, 3 - i, 2), valid)

        def body(way, unused):
            pl.when(way == 0)(lambda: relayed(0))
            pl.when(way == 1)(lambda: relayed(1))
            relay_attend(way)
            return unused

        lax.fori_loop(0, 3, body, 0)

        @pl.when(i == 0)
        def _():
            local_memory()

        @pl.when(i < ROUNDS)
        def _():
            scan_round(i)

        return unused

    lax.fori_loop(0, 8, iteration, 0)
    for kind in (2, 3):
        x_copy(13, kind, 0, 4).wait_recv()
    attend(0, 4, 2, sp >= 0)
    for number, lasts in enumerate(((4, 3), (3, 4), (3, 4), (3, 4), (3, 0))):
        for way, last in enumerate(lasts):
            for hop in range(1, last + 1):
                z_copy(number, way, hop, 0).wait_send()
    for number in range(9):
        for kind in range(4):
            x_copy(number, kind, 1, 0).wait_send()
    for number in range(10, 14):
        for kind in (2, 3):
            x_copy(number, kind, 0, 0).wait_send()
    for number in range(ROUNDS):
        scan_copy(number).wait_send()

    rooted = []
    for head in range(2):
        sides = []
        for side in range(2):
            part = acc[head, side * rows:(side + 1) * rows, :]
            sides.append(part / pltpu.roll(part, 64, 1))
        difference = sides[0] - lambdas[head] * sides[1]
        squared = jnp.where(low, 0.0, difference * difference)
        mean = jnp.sum(squared, axis=1, keepdims=True) * (1.0 / HEAD)
        rooted.append(difference * lax.rsqrt(mean + EPSILON))
    cat[:, 0:128] = (jnp.where(low, pltpu.roll(rooted[0], 64, 1), rooted[1])
                     * jnp.concatenate([head_gain[...]] * 2, axis=1)).astype(BF16)

    start_memory = jnp.zeros((HEAD, 128), F32)
    start_tail = jnp.zeros((8, 128), F32)
    entered = joined((start_memory, start_tail), (st_before[0:HEAD, :], st_before[HEAD:HEAD + 8, :]))
    memory_in, normal_in, stable_in = entered[0], entered[1][0:1], entered[1][1:2]
    spread = jnp.concatenate(
        [jnp.where(low_square, memory_in, 0.0), jnp.where(low_square, 0.0, memory_in)], axis=0)
    spread_normal = jnp.concatenate(
        [jnp.where(low_square, normal_in, 0.0), jnp.where(low_square, 0.0, normal_in)], axis=0)
    carried_log = gates[0] + stable_in
    row_top = jnp.maximum(carried_log, log_local[...])
    outside = jnp.exp(carried_log - row_top)
    inside = jnp.exp(log_local[...] - row_top)
    high, small = halves(spread)
    numerator = outside * (dot_t(mq[...], high) + dot_t(mq[...], small)) + inside * num_local[0]
    high, small = halves(spread_normal)
    denominator = outside * (dot_t(mq[...], high) + dot_t(mq[...], small)) + inside * num_local[1]
    cat[:, 128:256] = (numerator / jnp.maximum(jnp.abs(denominator), 1.0)).astype(BF16)

    for load in out_loads:
        load.wait()
    both = cat[...]

    def share(seat):
        return dot(both, wo[seat]).astype(BF16)

    offsets = (2, 1, 3, 0)
    pairs = []
    for number, offset in enumerate(offsets):
        to_partner[number] = share(2 * ((y + offset) % 4) + 1 - c)
        pairs.append(remote(to_partner.at[number], from_partner.at[number], pair_send.at[number],
                            pair_recv.at[number], sp, partner))
        pairs[number].start()

    def summed(number):
        own = share(2 * ((y + offsets[number]) % 4) + c).astype(F32)
        pairs[number].wait_recv()
        return own + from_partner[number].astype(F32)

    quarter = half_rows // 2

    def shift(number, seat, part=None):
        if part is None:
            source, target = to_ring.at[number], from_ring.at[number]
        else:
            span = pl.ds(part * quarter, quarter)
            source, target = to_ring.at[number, span, :], from_ring.at[number, span, :]
        lane_of = part or 0
        return remote(source, target, sum_send.at[number, lane_of], sum_recv.at[number, lane_of],
                      sp, seat)

    across_right = [shift(0, right, part) for part in range(2)]
    across_left = [shift(1, left, part) for part in range(2)]
    along_right, along_left = shift(2, right), shift(4, left)
    added_right = [shift(3, right, part) for part in range(2)]
    added_left = [shift(5, left, part) for part in range(2)]
    total = summed(0)
    to_ring[0] = total[:half_rows].astype(BF16)
    to_ring[1] = total[half_rows:].astype(BF16)
    for part in range(2):
        across_right[part].start()
        across_left[part].start()
    total = summed(1)
    to_ring[2] = total[half_rows:].astype(BF16)
    along_right.start()
    rest = total[:half_rows]
    total = summed(2)
    to_ring[4] = total[:half_rows].astype(BF16)
    along_left.start()
    other = total[half_rows:]
    total = summed(3)
    for part in range(2):
        span = slice(part * quarter, (part + 1) * quarter)
        across_right[part].wait_recv()
        to_ring[3, span, :] = (rest[span] + from_ring[0, span, :].astype(F32)).astype(BF16)
        added_right[part].start()
        across_left[part].wait_recv()
        to_ring[5, span, :] = (other[span] + from_ring[1, span, :].astype(F32)).astype(BF16)
        added_left[part].start()
    along_right.wait_recv()
    along_left.wait_recv()
    lower = total[half_rows:] + from_ring[2].astype(F32)
    upper = total[:half_rows] + from_ring[4].astype(F32)
    for part in range(2):
        span = slice(part * quarter, (part + 1) * quarter)
        added_right[part].wait_recv()
        out[span, :] = (upper[span] + from_ring[3, span, :].astype(F32)).astype(BF16)
        added_left[part].wait_recv()
        out[half_rows + part * quarter:half_rows + (part + 1) * quarter, :] = (
            lower[span] + from_ring[5, span, :].astype(F32)).astype(BF16)
    shifts = across_right + across_left + added_right + added_left + [along_right, along_left]
    for copy in pairs + shifts:
        copy.wait_send()


def per_device(
    inputs, norm_gain, query_weight, key_weight, value_weight, memory_query_weight,
    memory_key_weight, memory_value_weight, input_gate_weight, forget_gate_weight, forget_bias,
    decay_shift, lambdas, head_gain, out_weight_attention, out_weight_memory,
):
    rows, columns = inputs.shape
    middle = DD // 2
    inverse = 1.0 / ROTARY_BASE ** (np.arange(middle) / middle)
    near = np.tile(np.arange(rows)[:, None] * inverse[None, :], (1, 8))
    far = np.tile((np.arange(SPANS) * rows)[:, None] * inverse[None, :], (1, 8))
    near = jnp.asarray(np.stack([np.cos(near), np.sin(near)]), F32)
    far = jnp.asarray(np.stack([np.cos(far), np.sin(far)], axis=1), F32)
    vmem = pl.BlockSpec(memory_space=pltpu.VMEM)
    anywhere = pl.BlockSpec(memory_space=pl.ANY)
    half = rows // 2
    scratch = [
        pltpu.VMEM((8, 1, columns), F32),
        pltpu.VMEM((2, rows, 128), F32),
        pltpu.VMEM((2, 128), F32),
        pltpu.VMEM((2, 2048), BF16),
        pltpu.VMEM((2, 2048), BF16),
        pltpu.SMEM((2,), F32),
        pltpu.VMEM((2, rows), F32),
        pltpu.SMEM((2,), F32),
        pltpu.VMEM((1, HEAD), F32),
        pltpu.VMEM((8, rows, columns), BF16),
        pltpu.VMEM((8, rows, columns), BF16),
        pltpu.VMEM((rows, columns), F32),
        pltpu.VMEM((3, 2048, 256), BF16),
        pltpu.VMEM((8, 256, 256), BF16),
        pltpu.VMEM((2, SPANS, rows, 128), BF16),
        pltpu.VMEM((2, 2 * rows, 128), BF16),
        pltpu.VMEM((rows, 128), BF16),
        pltpu.VMEM((rows, 128), BF16),
        pltpu.VMEM((rows, 128), BF16),
        pltpu.VMEM((2, rows, 128), F32),
        pltpu.VMEM((2, rows), F32),
        pltpu.VMEM((2, 2 * rows, 128), F32),
        pltpu.VMEM((2, 2 * rows, 128), F32),
        pltpu.VMEM((ROUNDS, HEAD + 8, 128), F32),
        pltpu.VMEM((ROUNDS, HEAD + 8, 128), F32),
        pltpu.VMEM((HEAD + 8, 128), F32),
        pltpu.VMEM((2, rows, 128), F32),
        pltpu.VMEM((rows, 128), F32),
        pltpu.VMEM((rows, 256), BF16),
        pltpu.VMEM((4, rows, 256), BF16),
        pltpu.VMEM((4, rows, 256), BF16),
        pltpu.VMEM((6, half, 256), BF16),
        pltpu.VMEM((6, half, 256), BF16),
        pltpu.SemaphoreType.DMA((9,)),
        pltpu.SemaphoreType.DMA((25,)),
        pltpu.SemaphoreType.DMA((13,)),
        pltpu.SemaphoreType.DMA((13,)),
        pltpu.SemaphoreType.DMA((5, 2, 4)),
        pltpu.SemaphoreType.DMA((5, 2, 4)),
        pltpu.SemaphoreType.DMA((14, 4)),
        pltpu.SemaphoreType.DMA((14, 4)),
        pltpu.SemaphoreType.DMA((ROUNDS,)),
        pltpu.SemaphoreType.DMA((ROUNDS,)),
        pltpu.SemaphoreType.DMA((4,)),
        pltpu.SemaphoreType.DMA((4,)),
        pltpu.SemaphoreType.DMA((6, 2)),
        pltpu.SemaphoreType.DMA((6, 2)),
    ]
    return pl.pallas_call(
        layer_kernel,
        out_shape=jax.ShapeDtypeStruct((rows, columns), BF16),
        in_specs=[anywhere] * 18,
        out_specs=vmem,
        scratch_shapes=scratch,
        compiler_params=pltpu.CompilerParams(
            collective_id=0, has_side_effects=True, vmem_limit_bytes=60 * 1024 * 1024),
        name="layer",
    )(
        inputs, norm_gain.reshape(8, 1, 256), near, far, query_weight, key_weight, value_weight,
        memory_query_weight, memory_key_weight, memory_value_weight, input_gate_weight.T,
        forget_gate_weight.T, forget_bias, decay_shift.T, lambdas, head_gain.reshape(1, HEAD),
        out_weight_attention, out_weight_memory,
    )


def solution(mesh):
    split = P(None, "tp")
    placed = (
        P("sp", "tp"), P(), split, split, split, split, split, split, split, split,
        P("tp"), P("sp", "tp"), P("tp"), P(), P("tp", None), P("tp", None),
    )
    return jax.shard_map(
        per_device, mesh=mesh, in_specs=placed, out_specs=P("sp", "tp"), check_vma=False)
```

```python
import jax
import numpy as np
import jax.numpy as jnp
from jax import lax
from jax.experimental import pallas as pl
from jax.experimental.pallas import tpu as pltpu
from jax.sharding import PartitionSpec as P

HEAD = 64
DD = 32
EPSILON = 1e-06
ROTARY_BASE = 10000.0
NEGATIVE = -1e30
LOG2E = 1.4426950408889634
SPANS = 32
ROUNDS = 5
X_LAG = 2
RELAY_LAG = 1
MESH = pl.DeviceIdType.MESH
F32 = jnp.float32
BF16 = jnp.bfloat16


def dot(a, b):
    return jnp.dot(a, b, preferred_element_type=F32)


def dot_t(a, b):
    return lax.dot_general(a, b, (((1,), (1,)), ((), ())), preferred_element_type=F32)


def halves(a):
    high = a.astype(BF16)
    return high, (a - high.astype(F32)).astype(BF16)


def thirds(a):
    high = a.astype(BF16)
    rest = a - high.astype(F32)
    middle = rest.astype(BF16)
    return high, middle, (rest - middle.astype(F32)).astype(BF16)


def layer_kernel(
    x, gain_in, near_in, far_in, wq, wk, wv, wmq, wmk, wmv, wig_in, wfg_in, bias_in, decay_in,
    lambdas_in, head_gain_in, woa, wom, out,
    gain, near_table, far_table, wig, wfg, bias, decay, lambdas, head_gain,
    xg, xs, squares, w, wo, held, qs, mq, mk, mv, gates, gate_rows, acc, top, st_in, st_out, st_before,
    num_local, log_local, cat, to_partner, from_partner, to_ring, from_ring,
    small_sem, load_sem, gather_send, gather_recv, z_send, z_recv, x_send, x_recv, scan_send, scan_recv,
    pair_send, pair_recv, sum_send, sum_recv,
):
    rows = x.shape[0]
    half_rows = rows // 2
    sp = lax.axis_index("sp")
    tp = lax.axis_index("tp")
    y, c = tp // 2, tp % 2
    right = 2 * ((y + 1) % 4) + c
    left = 2 * ((y + 3) % 4) + c
    across = 2 * ((y + 2) % 4) + c
    partner = 2 * y + 1 - c
    z, across_x = sp // 4, sp % 4
    above, below = 4 * ((z + 1) % 8) + across_x, 4 * ((z + 7) % 8) + across_x
    nexts = [above, below, 4 * z + (across_x + 1) % 4, 4 * z + (across_x + 3) % 4]

    def span_at(dz, dx):
        return 4 * ((z + dz + 16) % 8) + (across_x + dx) % 4

    def remote(src, dst, send, recv, span, seat):
        return pltpu.make_async_remote_copy(
            src_ref=src, dst_ref=dst, send_sem=send, recv_sem=recv,
            device_id=(span, seat), device_id_type=MESH)

    barrier = pltpu.get_barrier_semaphore()
    greeted = [(sp, right), (sp, left), (sp, partner)] + [(span, tp) for span in nexts]
    for span, seat in greeted:
        pl.semaphore_signal(barrier, inc=1, device_id=(span, seat), device_id_type=MESH)

    own_load = pltpu.make_async_copy(x, xg.at[tp], load_sem.at[0])
    own_load.start()
    loads = []
    for number, (weight, tile, at) in enumerate(
            ((wq, 0, 0), (wk, 0, 128), (wv, 1, 0), (wmq, 1, 128), (wmk, 2, 0), (wmv, 2, 128))):
        loads.append(pltpu.make_async_copy(
            weight, w.at[tile, :, pl.ds(at, 128)], load_sem.at[1 + number]))
    small_loads = {}
    for number, (source, target) in enumerate((
            (gain_in, gain), (near_in, near_table), (far_in.at[sp], far_table), (wig_in, wig),
            (wfg_in, wfg), (bias_in, bias), (decay_in, decay), (lambdas_in, lambdas),
            (head_gain_in, head_gain))):
        small_loads[number] = pltpu.make_async_copy(source, target, small_sem.at[number])
        small_loads[number].start()
    for load in loads:
        load.start()
    out_loads = []
    for j in range(8):
        for part, weight in enumerate((woa, wom)):
            out_loads.append(pltpu.make_async_copy(
                weight.at[:, pl.ds(256 * j, 256)], wo.at[j, pl.ds(128 * part, 128), :],
                load_sem.at[9 + 2 * j + part]))
    for load in out_loads:
        load.start()

    def piece(seat, half):
        return xg.at[seat, pl.ds(half * half_rows, half_rows), :]

    def gather(number, ref, seat):
        return remote(ref, ref, gather_send.at[number], gather_recv.at[number], sp, seat)

    sends = {
        0: gather(0, piece(tp, 0), right),
        1: gather(1, piece(tp, 1), right),
        2: gather(2, piece(tp, 1), left),
        3: gather(3, piece(tp, 0), left),
        4: gather(4, xg.at[tp], partner),
        5: gather(5, piece(left, 0), right),
        6: gather(6, piece(left, 0), partner),
        7: gather(7, piece(right, 1), left),
        8: gather(8, piece(right, 1), partner),
        9: gather(9, piece(left, 1), partner),
        10: gather(10, piece(right, 0), partner),
        11: gather(11, piece(across, 0), partner),
        12: gather(12, piece(across, 1), partner),
    }
    own_load.wait()
    pl.semaphore_wait(barrier, len(greeted))
    for number in (0, 2, 1, 3, 4):
        sends[number].start()

    def absorb(seat):
        block = xg[seat].astype(F32)
        squares[...] += block * block
        xs[seat] = (block * gain[seat]).astype(BF16)

    squares[...] = jnp.zeros_like(squares)
    small_loads[0].wait()
    absorb(tp)
    sends[0].wait_recv()
    sends[5].start()
    sends[6].start()
    sends[2].wait_recv()
    sends[7].start()
    sends[8].start()
    sends[4].wait_recv()
    absorb(partner)
    sends[1].wait_recv()
    sends[9].start()
    sends[3].wait_recv()
    sends[10].start()
    absorb(left)
    absorb(right)
    sends[5].wait_recv()
    sends[11].start()
    sends[7].wait_recv()
    sends[12].start()
    for number in (6, 8, 9, 10):
        sends[number].wait_recv()
    absorb(2 * ((y + 1) % 4) + 1 - c)
    absorb(2 * ((y + 3) % 4) + 1 - c)
    absorb(across)
    sends[11].wait_recv()
    sends[12].wait_recv()
    absorb(2 * ((y + 2) % 4) + 1 - c)
    for number in range(13):
        sends[number].wait_send()
    for load in loads + [small_loads[number] for number in range(1, 9)]:
        load.wait()

    inverse = lax.rsqrt(
        jnp.sum(squares[...], axis=1, keepdims=True) * (1.0 / 2048.0) + EPSILON)
    scaled = jnp.concatenate([xs[j] for j in range(8)], axis=1)
    lane = lax.broadcasted_iota(jnp.int32, (rows, 128), 1)
    low = lane < HEAD
    former = lane % 32 < 16

    far_cosine, far_sine = far_table[0:1, :], far_table[1:2, :]
    cosine = far_cosine * near_table[0] - far_sine * near_table[1]
    sine = far_sine * near_table[0] + far_cosine * near_table[1]
    sine = jnp.where(former, -sine, sine)

    def rotated(flat):
        floats = flat.astype(BF16).astype(F32)
        swapped = jnp.where(former, pltpu.roll(floats, 112, 1), pltpu.roll(floats, 16, 1))
        return (floats * cosine + swapped * sine).astype(BF16).astype(F32)

    product = dot(scaled, w[0]) * inverse
    queries = rotated(product[:, :128])
    keys = rotated(product[:, 128:])
    product = dot(scaled, w[1]) * inverse
    values = product[:, :128].astype(BF16).astype(F32)
    mq[...] = product[:, 128:].astype(BF16)
    held[0, sp] = jnp.where(low, keys, pltpu.roll(values, 64, 1)).astype(BF16)
    held[1, sp] = jnp.where(low, pltpu.roll(keys, 64, 1), values).astype(BF16)
    def z_copy(chain, way, hop, dx):
        dz = 1 - hop if way == 0 else hop - 1
        ref = held.at[1 if isinstance(chain, int) and chain == 0 else 0, span_at(dz, dx)]
        return remote(ref, ref, z_send.at[chain, way, hop - 1], z_recv.at[chain, way, hop - 1],
                      nexts[way], tp)

    def x_copy(number, kind, ring, dz):
        if kind < 2:
            ref = held.at[ring, span_at(dz, 0)]
        else:
            ref = held.at[ring, span_at(dz, 3 if kind == 2 else 1),
                          pl.ds((kind - 2) * half_rows, half_rows), :]
        return remote(ref, ref, x_send.at[number, kind], x_recv.at[number, kind],
                      nexts[2 + kind % 2], tp)

    for way in range(2):
        z_copy(0, way, 1, 0).start()
        x_copy(5, way, 0, 0).start()
    for way in range(2):
        z_copy(1, way, 1, 0).start()
        x_copy(0, way, 1, 0).start()

    for head in range(2):
        turned = queries if head == 0 else pltpu.roll(queries, 64, 1)
        for side in range(2):
            inside = (lane >= DD * side) & (lane < DD * side + DD)
            qs[head, side * rows:(side + 1) * rows, :] = jnp.where(inside, turned, 0.0).astype(BF16)
    product = dot(scaled, w[2]) * inverse
    mk[...] = product[:, :128].astype(BF16)
    mv[...] = product[:, 128:].astype(BF16)
    inverse_row = jnp.transpose(jnp.broadcast_to(inverse, (rows, 128)))[0:1, :]
    gate_in = dot_t(wig[...], scaled) * inverse_row
    forget = dot_t(wfg[...], scaled) * inverse_row

    def log_sigmoid(a):
        return jnp.minimum(a, 0.0) - jnp.log1p(jnp.exp(-jnp.abs(a)))

    def per_head(parts):
        return jnp.where(low, parts[0], parts[1])

    first_row = lax.broadcasted_iota(jnp.int32, (2, rows), 0) == 0
    log_forget = log_sigmoid(forget + jnp.where(first_row, bias[0], bias[1])) + decay[...]
    before_or_at = (lax.broadcasted_iota(jnp.int32, (rows, rows), 1)
                    <= lax.broadcasted_iota(jnp.int32, (rows, rows), 0))
    triangle = jnp.where(before_or_at, 1.0, 0.0).astype(BF16)
    high, middle, small = thirds(log_forget)
    cumulative = dot_t(high, triangle) + dot_t(middle, triangle) + dot_t(small, triangle)
    gate_rows[...] = gate_in - cumulative
    upper_rows = lax.broadcasted_iota(jnp.int32, (128, rows), 0) < HEAD

    def columns(pair):
        return jnp.transpose(jnp.where(upper_rows, pair[0:1, :], pair[1:2, :]))

    gates[0] = columns(cumulative)
    gates[1] = columns(gate_rows[...])
    span_decay = gates[0, rows - 1:rows, :]
    toward_end = span_decay + gates[1]
    span_top = jnp.max(toward_end, axis=0, keepdims=True)
    end_weights = jnp.exp(toward_end - span_top)
    key_floats = mk[...].astype(F32) * 0.125
    weighted = jnp.transpose(end_weights * mv[...].astype(F32))
    high, small = halves(weighted)
    keys_exact = key_floats.astype(BF16)
    outer = dot(high, keys_exact) + dot(small, keys_exact)
    row = lax.broadcasted_iota(jnp.int32, (8, 128), 0)

    def tail(normal, stable, decays):
        return jnp.where(row == 0, normal, jnp.where(row == 1, stable, decays))

    low_square = low[:HEAD]
    st_out[0, 0:HEAD, :] = jnp.where(low_square, outer[:HEAD], outer[HEAD:])
    st_out[0, HEAD:HEAD + 8, :] = tail(
        jnp.sum(end_weights * key_floats, axis=0, keepdims=True), span_top, span_decay)
    for kind in range(2):
        st_before[kind, 0:HEAD, :] = jnp.zeros((HEAD, 128), F32)
        st_before[kind, HEAD:HEAD + 8, :] = tail(0.0, NEGATIVE, 0.0) + jnp.zeros((8, 128), F32)

    def rise(number):
        return jnp.where(number == 2, 1, jnp.where(number == 3, 2, 4))

    def scan_copy(number):
        beside = jnp.where(number == 0, across_x + 1 - 2 * (across_x % 2), (across_x + 2) % 4)
        target = jnp.where(number < 2, 4 * z + beside, 4 * ((z + rise(number)) % 8) + across_x)
        return remote(st_out.at[number], st_in.at[number], scan_send.at[number],
                      scan_recv.at[number], target, tp)

    def joined(earlier, later):
        old, new = earlier[1], later[1]
        decays, stable, later_stable = new[2:3], old[1:2], new[1:2]
        highest = jnp.maximum(decays + stable, later_stable)
        first = jnp.exp(decays + stable - highest)
        second = jnp.exp(later_stable - highest)
        return (first * earlier[0] + second * later[0],
                tail(first * old[0:1] + second * new[0:1], highest, old[2:3] + decays))

    scale = DD ** (-0.5) * LOG2E
    ones_low = low

    def visit(ring, position, mask=None):
        block = held[ring, position]
        extended = jnp.where(ones_low, jnp.ones_like(block), block)
        scores = dot_t(qs[ring], block)
        if mask is not None:
            scores = jnp.where(mask, scores, NEGATIVE)
            highest = jnp.broadcast_to(jnp.max(scores, axis=1, keepdims=True), (2 * rows, 128))
        else:
            old = top[ring]
            highest = jnp.maximum(old, jnp.max(scores, axis=1, keepdims=True))
        shift = highest * scale
        weights = jnp.exp2(scores * scale - jnp.concatenate([shift] * (rows // 128), axis=1))
        product = dot(weights.astype(BF16), extended)
        if mask is not None:
            acc[ring] = product
        else:
            acc[ring] = acc[ring] * jnp.exp2((old - highest) * scale) + product
        top[ring] = highest

    causal = jnp.concatenate([before_or_at, before_or_at], axis=0)
    visit(0, sp, causal)
    scan_copy(0).start()
    x_copy(5, 0, 0, 0).wait_recv()
    x_copy(5, 2, 0, 0).start()
    for way in range(2):
        z_copy(2, way, 1, 3).start()
    x_copy(5, 1, 0, 0).wait_recv()
    x_copy(5, 3, 0, 0).start()
    for way in range(2):
        z_copy(3, way, 1, 1).start()
    visit(1, sp, causal)

    def local_memory():
        sums, tops, totals = [], [], []
        for head in range(2):
            inside = low if head == 0 else ~low
            gap = gates[0, :, HEAD * head:HEAD * head + 1] + gate_rows[head:head + 1, :]
            gap = jnp.where(before_or_at, gap, NEGATIVE)
            highest = jnp.max(gap, axis=1, keepdims=True)
            within = jnp.exp(gap - highest)
            mine = jnp.where(inside, mq[...].astype(F32), 0.0).astype(BF16)
            scores = within * (dot_t(mine, mk[...]) * 0.125)
            high, small = halves(scores)
            sums.append(dot(high, mv[...]) + dot(small, mv[...]))
            totals.append(jnp.sum(scores, axis=1, keepdims=True))
            tops.append(highest)
        num_local[0] = per_head(sums)
        num_local[1] = per_head(totals) + jnp.zeros((rows, 128), F32)
        log_local[...] = per_head(tops) + jnp.zeros((rows, 128), F32)

    def scan_round(number):
        scan_copy(number).wait_recv()
        memory = st_in[number, 0:HEAD, :]
        ending = st_in[number, HEAD:HEAD + 8, :]
        in_row = number < 2
        later_half = jnp.where(number == 0, across_x % 2, across_x // 2)
        earlier = jnp.where(in_row, later_half, jnp.where(z >= rise(number), 1, 0)) > 0
        kind = jnp.where(in_row, 0, 1)

        @pl.when(earlier)
        def _():
            done = joined((memory, ending),
                          (st_before[kind, 0:HEAD, :], st_before[kind, HEAD:HEAD + 8, :]))
            st_before[kind, 0:HEAD, :] = done[0]
            st_before[kind, HEAD:HEAD + 8, :] = done[1]

        @pl.when(number < ROUNDS - 1)
        def _():
            mine = (st_out[number, 0:HEAD, :], st_out[number, HEAD:HEAD + 8, :])
            after = joined((memory, ending), mine)
            ahead = joined(mine, (memory, ending))
            for place, (one, two, same) in enumerate(zip(after, ahead, mine)):
                merged = jnp.where(earlier, one, jnp.where(in_row, two, same))
                st_out[number + 1, HEAD * place:HEAD + 8 * place, :] = merged

    def attend(ring, dz, dx, valid):
        origin = span_at(dz, dx)

        @pl.when(valid & (origin < sp))
        def _():
            visit(ring, origin)

    def iteration(i, unused):
        pair, hop = i % 2, i // 2 + 1

        def by_way(ups, downs, then):
            def body(way, unused):
                pl.when(way == 0)(ups)
                pl.when(way == 1)(downs)
                then(way)
                return unused

            lax.fori_loop(0, 2, body, 0)

        def signed(way, distance):
            return (2 * way - 1) * distance

        @pl.when((i >= 1) & (i < ROUNDS))
        def _():
            scan_copy(i).start()

        def own_chain(way):
            last = 4 - way

            @pl.when(i < last)
            def _():
                z_copy(0, way, i + 1, 0).wait_recv()

                @pl.when(i < last - 1)
                def _():
                    z_copy(0, way, i + 2, 0).start()

                for kind in range(2):
                    x_copy(5 * way + i + 1, kind, 1, (2 * way - 1) * (i + 1)).start()

        by_way(lambda: own_chain(0), lambda: own_chain(1),
               lambda way: attend(1, signed(way, i + 1), 0, i < 4 - way))

        def x_arrival(rows_way, kind):
            valid = (i <= 4) if rows_way == 0 else (i >= 1) & (i <= 3)

            @pl.when(valid)
            def _():
                dz = (2 * rows_way - 1) * i
                x_copy(5 * rows_way + i, kind, 1, dz).wait_recv()
                x_copy(5 * rows_way + i, kind + 2, 1, dz).start()

        def x_attend(rows_way, side):
            j = i - X_LAG
            valid = (j >= 0) & (j <= 4) if rows_way == 0 else (j >= 1) & (j <= 3)
            attend(1, (2 * rows_way - 1) * j, 3 - 2 * side, valid)

        by_way(lambda: x_arrival(0, 0), lambda: x_arrival(0, 1), lambda side: x_attend(0, side))

        @pl.when(i == 0)
        def _():
            x_copy(5, 2, 0, 0).wait_recv()
            x_copy(5, 3, 0, 0).wait_recv()
            for way in range(2):
                z_copy(4, way, 1, 2).start()

        def chain(number, way, dx, last):
            @pl.when(hop <= last)
            def _():
                z_copy(number, way, hop, dx).wait_recv()

                @pl.when(hop < last)
                def _():
                    z_copy(number, way, hop + 1, dx).start()

        first = 1 + 2 * pair

        by_way(lambda: chain(first, 0, pair, 4), lambda: chain(first, 1, pair, 3),
               lambda way: attend(0, signed(way, hop), pair, hop <= 4 - way))
        by_way(lambda: x_arrival(1, 0), lambda: x_arrival(1, 1), lambda side: x_attend(1, side))
        by_way(lambda: chain(first + 1, 0, 3 - pair, 3), lambda: chain(first + 1, 1, 3 - pair, 4),
               lambda way: attend(0, signed(way, hop), 3 - pair, hop <= 3 + way))

        def relayed(rows_way):
            j = i - 1
            valid = (j >= 0) & (j <= 4) if rows_way == 0 else (j >= 1) & (j <= 3)

            @pl.when(valid)
            def _():
                for kind in (2, 3):
                    x_copy(5 * rows_way + j, kind, 1, (2 * rows_way - 1) * j).wait_recv()

        def relay_attend(way):
            j = i - 1 - RELAY_LAG
            own = way == 2
            valid = jnp.where(own, i < 3, (j >= way) & (j <= 4 - way))
            attend(jnp.where(own, 0, 1), jnp.where(own, 0, signed(way, j)),
                   jnp.where(own, 3 - i, 2), valid)

        def body(way, unused):
            pl.when(way == 0)(lambda: relayed(0))
            pl.when(way == 1)(lambda: relayed(1))
            relay_attend(way)
            return unused

        lax.fori_loop(0, 3, body, 0)

        @pl.when(i == 0)
        def _():
            local_memory()

        @pl.when(i < ROUNDS)
        def _():
            scan_round(i)

        return unused

    lax.fori_loop(0, 8, iteration, 0)
    for number, lasts in enumerate(((4, 3), (4, 3), (3, 4), (4, 3), (3, 4))):
        for way, last in enumerate(lasts):
            for hop in range(1, last + 1):
                z_copy(number, way, hop, 0).wait_send()
    for number in range(9):
        for kind in range(4):
            x_copy(number, kind, 1, 0).wait_send()
    for number in range(ROUNDS):
        scan_copy(number).wait_send()

    rooted = []
    for head in range(2):
        sides = []
        for side in range(2):
            part = acc[head, side * rows:(side + 1) * rows, :]
            sides.append(part / pltpu.roll(part, 64, 1))
        difference = sides[0] - lambdas[head] * sides[1]
        squared = jnp.where(low, 0.0, difference * difference)
        mean = jnp.sum(squared, axis=1, keepdims=True) * (1.0 / HEAD)
        rooted.append(difference * lax.rsqrt(mean + EPSILON))
    cat[:, 0:128] = (jnp.where(low, pltpu.roll(rooted[0], 64, 1), rooted[1])
                     * jnp.concatenate([head_gain[...]] * 2, axis=1)).astype(BF16)

    start_memory = jnp.zeros((HEAD, 128), F32)
    start_tail = jnp.zeros((8, 128), F32)
    entered = (start_memory, start_tail)
    for kind in (1, 0):
        entered = joined(entered, (st_before[kind, 0:HEAD, :], st_before[kind, HEAD:HEAD + 8, :]))
    memory_in, normal_in, stable_in = entered[0], entered[1][0:1], entered[1][1:2]
    spread = jnp.concatenate(
        [jnp.where(low_square, memory_in, 0.0), jnp.where(low_square, 0.0, memory_in)], axis=0)
    spread_normal = jnp.concatenate(
        [jnp.where(low_square, normal_in, 0.0), jnp.where(low_square, 0.0, normal_in)], axis=0)
    carried_log = gates[0] + stable_in
    row_top = jnp.maximum(carried_log, log_local[...])
    outside = jnp.exp(carried_log - row_top)
    inside = jnp.exp(log_local[...] - row_top)
    high, small = halves(spread)
    numerator = outside * (dot_t(mq[...], high) + dot_t(mq[...], small)) + inside * num_local[0]
    high, small = halves(spread_normal)
    denominator = outside * (dot_t(mq[...], high) + dot_t(mq[...], small)) + inside * num_local[1]
    cat[:, 128:256] = (numerator / jnp.maximum(jnp.abs(denominator), 1.0)).astype(BF16)

    for load in out_loads:
        load.wait()
    both = cat[...]

    def share(seat):
        return dot(both, wo[seat]).astype(BF16)

    offsets = (2, 1, 3, 0)
    pairs = []
    for number, offset in enumerate(offsets):
        to_partner[number] = share(2 * ((y + offset) % 4) + 1 - c)
        pairs.append(remote(to_partner.at[number], from_partner.at[number], pair_send.at[number],
                            pair_recv.at[number], sp, partner))
        pairs[number].start()

    def summed(number):
        own = share(2 * ((y + offsets[number]) % 4) + c).astype(F32)
        pairs[number].wait_recv()
        return own + from_partner[number].astype(F32)

    quarter = half_rows // 2

    def shift(number, seat, part=None):
        if part is None:
            source, target = to_ring.at[number], from_ring.at[number]
        else:
            span = pl.ds(part * quarter, quarter)
            source, target = to_ring.at[number, span, :], from_ring.at[number, span, :]
        lane_of = part or 0
        return remote(source, target, sum_send.at[number, lane_of], sum_recv.at[number, lane_of],
                      sp, seat)

    across_right = [shift(0, right, part) for part in range(2)]
    across_left = [shift(1, left, part) for part in range(2)]
    along_right, along_left = shift(2, right), shift(4, left)
    added_right = [shift(3, right, part) for part in range(2)]
    added_left = [shift(5, left, part) for part in range(2)]
    total = summed(0)
    to_ring[0] = total[:half_rows].astype(BF16)
    to_ring[1] = total[half_rows:].astype(BF16)
    for part in range(2):
        across_right[part].start()
        across_left[part].start()
    total = summed(1)
    to_ring[2] = total[half_rows:].astype(BF16)
    along_right.start()
    rest = total[:half_rows]
    total = summed(2)
    to_ring[4] = total[:half_rows].astype(BF16)
    along_left.start()
    other = total[half_rows:]
    total = summed(3)
    for part in range(2):
        span = slice(part * quarter, (part + 1) * quarter)
        across_right[part].wait_recv()
        to_ring[3, span, :] = (rest[span] + from_ring[0, span, :].astype(F32)).astype(BF16)
        added_right[part].start()
        across_left[part].wait_recv()
        to_ring[5, span, :] = (other[span] + from_ring[1, span, :].astype(F32)).astype(BF16)
        added_left[part].start()
    along_right.wait_recv()
    along_left.wait_recv()
    lower = total[half_rows:] + from_ring[2].astype(F32)
    upper = total[:half_rows] + from_ring[4].astype(F32)
    for part in range(2):
        span = slice(part * quarter, (part + 1) * quarter)
        added_right[part].wait_recv()
        out[span, :] = (upper[span] + from_ring[3, span, :].astype(F32)).astype(BF16)
        added_left[part].wait_recv()
        out[half_rows + part * quarter:half_rows + (part + 1) * quarter, :] = (
            lower[span] + from_ring[5, span, :].astype(F32)).astype(BF16)
    shifts = across_right + across_left + added_right + added_left + [along_right, along_left]
    for copy in pairs + shifts:
        copy.wait_send()


def per_device(
    inputs, norm_gain, query_weight, key_weight, value_weight, memory_query_weight,
    memory_key_weight, memory_value_weight, input_gate_weight, forget_gate_weight, forget_bias,
    decay_shift, lambdas, head_gain, out_weight_attention, out_weight_memory,
):
    rows, columns = inputs.shape
    middle = DD // 2
    inverse = 1.0 / ROTARY_BASE ** (np.arange(middle) / middle)
    near = np.tile(np.arange(rows)[:, None] * inverse[None, :], (1, 8))
    far = np.tile((np.arange(SPANS) * rows)[:, None] * inverse[None, :], (1, 8))
    near = jnp.asarray(np.stack([np.cos(near), np.sin(near)]), F32)
    far = jnp.asarray(np.stack([np.cos(far), np.sin(far)], axis=1), F32)
    vmem = pl.BlockSpec(memory_space=pltpu.VMEM)
    anywhere = pl.BlockSpec(memory_space=pl.ANY)
    half = rows // 2
    scratch = [
        pltpu.VMEM((8, 1, columns), F32),
        pltpu.VMEM((2, rows, 128), F32),
        pltpu.VMEM((2, 128), F32),
        pltpu.VMEM((2, 2048), BF16),
        pltpu.VMEM((2, 2048), BF16),
        pltpu.SMEM((2,), F32),
        pltpu.VMEM((2, rows), F32),
        pltpu.SMEM((2,), F32),
        pltpu.VMEM((1, HEAD), F32),
        pltpu.VMEM((8, rows, columns), BF16),
        pltpu.VMEM((8, rows, columns), BF16),
        pltpu.VMEM((rows, columns), F32),
        pltpu.VMEM((3, 2048, 256), BF16),
        pltpu.VMEM((8, 256, 256), BF16),
        pltpu.VMEM((2, SPANS, rows, 128), BF16),
        pltpu.VMEM((2, 2 * rows, 128), BF16),
        pltpu.VMEM((rows, 128), BF16),
        pltpu.VMEM((rows, 128), BF16),
        pltpu.VMEM((rows, 128), BF16),
        pltpu.VMEM((2, rows, 128), F32),
        pltpu.VMEM((2, rows), F32),
        pltpu.VMEM((2, 2 * rows, 128), F32),
        pltpu.VMEM((2, 2 * rows, 128), F32),
        pltpu.VMEM((ROUNDS, HEAD + 8, 128), F32),
        pltpu.VMEM((ROUNDS, HEAD + 8, 128), F32),
        pltpu.VMEM((2, HEAD + 8, 128), F32),
        pltpu.VMEM((2, rows, 128), F32),
        pltpu.VMEM((rows, 128), F32),
        pltpu.VMEM((rows, 256), BF16),
        pltpu.VMEM((4, rows, 256), BF16),
        pltpu.VMEM((4, rows, 256), BF16),
        pltpu.VMEM((6, half, 256), BF16),
        pltpu.VMEM((6, half, 256), BF16),
        pltpu.SemaphoreType.DMA((9,)),
        pltpu.SemaphoreType.DMA((25,)),
        pltpu.SemaphoreType.DMA((13,)),
        pltpu.SemaphoreType.DMA((13,)),
        pltpu.SemaphoreType.DMA((5, 2, 4)),
        pltpu.SemaphoreType.DMA((5, 2, 4)),
        pltpu.SemaphoreType.DMA((10, 4)),
        pltpu.SemaphoreType.DMA((10, 4)),
        pltpu.SemaphoreType.DMA((ROUNDS,)),
        pltpu.SemaphoreType.DMA((ROUNDS,)),
        pltpu.SemaphoreType.DMA((4,)),
        pltpu.SemaphoreType.DMA((4,)),
        pltpu.SemaphoreType.DMA((6, 2)),
        pltpu.SemaphoreType.DMA((6, 2)),
    ]
    return pl.pallas_call(
        layer_kernel,
        out_shape=jax.ShapeDtypeStruct((rows, columns), BF16),
        in_specs=[anywhere] * 18,
        out_specs=vmem,
        scratch_shapes=scratch,
        compiler_params=pltpu.CompilerParams(
            collective_id=0, has_side_effects=True, vmem_limit_bytes=60 * 1024 * 1024),
        name="layer",
    )(
        inputs, norm_gain.reshape(8, 1, 256), near, far, query_weight, key_weight, value_weight,
        memory_query_weight, memory_key_weight, memory_value_weight, input_gate_weight.T,
        forget_gate_weight.T, forget_bias, decay_shift.T, lambdas, head_gain.reshape(1, HEAD),
        out_weight_attention, out_weight_memory,
    )


def solution(mesh):
    split = P(None, "tp")
    placed = (
        P("sp", "tp"), P(), split, split, split, split, split, split, split, split,
        P("tp"), P("sp", "tp"), P("tp"), P(), P("tp", None), P("tp", None),
    )
    return jax.shard_map(
        per_device, mesh=mesh, in_specs=placed, out_specs=P("sp", "tp"), check_vma=False)
```

```python
import jax
import numpy as np
import jax.numpy as jnp
from jax import lax
from jax.experimental import pallas as pl
from jax.experimental.pallas import tpu as pltpu
from jax.sharding import PartitionSpec as P

HEAD = 64
DD = 32
EPSILON = 1e-06
ROTARY_BASE = 10000.0
NEGATIVE = -1e30
LOG2E = 1.4426950408889634
SPANS = 32
ROUNDS = 5
X_LAG = 1
RELAY_LAG = 0
MESH = pl.DeviceIdType.MESH
F32 = jnp.float32
BF16 = jnp.bfloat16


def dot(a, b):
    return jnp.dot(a, b, preferred_element_type=F32)


def dot_t(a, b):
    return lax.dot_general(a, b, (((1,), (1,)), ((), ())), preferred_element_type=F32)


def halves(a):
    high = a.astype(BF16)
    return high, (a - high.astype(F32)).astype(BF16)


def thirds(a):
    high = a.astype(BF16)
    rest = a - high.astype(F32)
    middle = rest.astype(BF16)
    return high, middle, (rest - middle.astype(F32)).astype(BF16)


def layer_kernel(
    x, gain_in, near_in, far_in, wq, wk, wv, wmq, wmk, wmv, wig_in, wfg_in, bias_in, decay_in,
    lambdas_in, head_gain_in, woa, wom, out,
    gain, near_table, far_table, wig, wfg, bias, decay, lambdas, head_gain,
    xg, xs, squares, w, wo, held, qs, mq, mk, mv, gates, gate_rows, acc, top, st_in, st_out, st_before,
    num_local, log_local, cat, to_partner, from_partner, to_ring, from_ring,
    small_sem, load_sem, gather_send, gather_recv, z_send, z_recv, x_send, x_recv, scan_send, scan_recv,
    pair_send, pair_recv, sum_send, sum_recv,
):
    rows = x.shape[0]
    half_rows = rows // 2
    sp = lax.axis_index("sp")
    tp = lax.axis_index("tp")
    y, c = tp // 2, tp % 2
    right = 2 * ((y + 1) % 4) + c
    left = 2 * ((y + 3) % 4) + c
    across = 2 * ((y + 2) % 4) + c
    partner = 2 * y + 1 - c
    z, across_x = sp // 4, sp % 4
    above, below = 4 * ((z + 1) % 8) + across_x, 4 * ((z + 7) % 8) + across_x
    nexts = [above, below, 4 * z + (across_x + 1) % 4, 4 * z + (across_x + 3) % 4]

    def span_at(dz, dx):
        return 4 * ((z + dz + 16) % 8) + (across_x + dx) % 4

    def remote(src, dst, send, recv, span, seat):
        return pltpu.make_async_remote_copy(
            src_ref=src, dst_ref=dst, send_sem=send, recv_sem=recv,
            device_id=(span, seat), device_id_type=MESH)

    barrier = pltpu.get_barrier_semaphore()
    greeted = [(sp, right), (sp, left), (sp, partner)] + [(span, tp) for span in nexts]
    for span, seat in greeted:
        pl.semaphore_signal(barrier, inc=1, device_id=(span, seat), device_id_type=MESH)

    own_load = pltpu.make_async_copy(x, xg.at[tp], load_sem.at[0])
    own_load.start()
    loads = []
    for number, (weight, tile, at) in enumerate(
            ((wq, 0, 0), (wk, 0, 128), (wv, 1, 0), (wmq, 1, 128), (wmk, 2, 0), (wmv, 2, 128))):
        loads.append(pltpu.make_async_copy(
            weight, w.at[tile, :, pl.ds(at, 128)], load_sem.at[1 + number]))
    small_loads = {}
    for number, (source, target) in enumerate((
            (gain_in, gain), (near_in, near_table), (far_in.at[sp], far_table), (wig_in, wig),
            (wfg_in, wfg), (bias_in, bias), (decay_in, decay), (lambdas_in, lambdas),
            (head_gain_in, head_gain))):
        small_loads[number] = pltpu.make_async_copy(source, target, small_sem.at[number])
        small_loads[number].start()
    for load in loads:
        load.start()
    out_loads = []
    for j in range(8):
        for part, weight in enumerate((woa, wom)):
            out_loads.append(pltpu.make_async_copy(
                weight.at[:, pl.ds(256 * j, 256)], wo.at[j, pl.ds(128 * part, 128), :],
                load_sem.at[9 + 2 * j + part]))
    for load in out_loads:
        load.start()

    quarter = half_rows // 2

    def piece(seat, half, part=None):
        if part is None:
            return xg.at[seat, pl.ds(half * half_rows, half_rows), :]
        return xg.at[seat, pl.ds(half * half_rows + part * quarter, quarter), :]

    def gather(number, seat, goal, half=None):
        if half is None:
            ref = xg.at[seat]
            return [remote(ref, ref, gather_send.at[number, 0], gather_recv.at[number, 0], sp, goal)]
        if number in (1, 3, 6, 8, 9, 10):
            ref = piece(seat, half)
            return [remote(ref, ref, gather_send.at[number, 0], gather_recv.at[number, 0], sp, goal)]
        refs = [piece(seat, half, part) for part in range(2)]
        return [remote(ref, ref, gather_send.at[number, part], gather_recv.at[number, part], sp, goal)
                for part, ref in enumerate(refs)]

    sends = {
        0: gather(0, tp, right, 0),
        1: gather(1, tp, right, 1),
        2: gather(2, tp, left, 1),
        3: gather(3, tp, left, 0),
        4: gather(4, tp, partner),
        5: gather(5, left, right, 0),
        6: gather(6, left, partner, 0),
        7: gather(7, right, left, 1),
        8: gather(8, right, partner, 1),
        9: gather(9, left, partner, 1),
        10: gather(10, right, partner, 0),
        11: gather(11, across, partner, 0),
        12: gather(12, across, partner, 1),
    }
    own_load.wait()
    pl.semaphore_wait(barrier, len(greeted))
    for part in range(2):
        sends[0][part].start()
        sends[2][part].start()
    for number in (1, 3, 4):
        sends[number][0].start()

    def absorb(seat):
        block = xg[seat].astype(F32)
        squares[...] += block * block
        xs[seat] = (block * gain[seat]).astype(BF16)

    squares[...] = jnp.zeros_like(squares)
    small_loads[0].wait()
    absorb(tp)
    for part in range(2):
        sends[0][part].wait_recv()
        sends[5][part].start()
        sends[2][part].wait_recv()
        sends[7][part].start()
    sends[6][0].start()
    sends[8][0].start()
    sends[4][0].wait_recv()
    absorb(partner)
    sends[1][0].wait_recv()
    sends[9][0].start()
    sends[3][0].wait_recv()
    sends[10][0].start()
    absorb(left)
    absorb(right)
    for part in range(2):
        sends[5][part].wait_recv()
        sends[11][part].start()
        sends[7][part].wait_recv()
        sends[12][part].start()
    for number in (6, 8, 9, 10):
        sends[number][0].wait_recv()
    absorb(2 * ((y + 1) % 4) + 1 - c)
    absorb(2 * ((y + 3) % 4) + 1 - c)
    absorb(across)
    for part in range(2):
        sends[11][part].wait_recv()
        sends[12][part].wait_recv()
    absorb(2 * ((y + 2) % 4) + 1 - c)
    for number in range(13):
        for copy in sends[number]:
            copy.wait_send()
    for load in loads + [small_loads[number] for number in range(1, 9)]:
        load.wait()

    inverse = lax.rsqrt(
        jnp.sum(squares[...], axis=1, keepdims=True) * (1.0 / 2048.0) + EPSILON)
    scaled = jnp.concatenate([xs[j] for j in range(8)], axis=1)
    lane = lax.broadcasted_iota(jnp.int32, (rows, 128), 1)
    low = lane < HEAD
    former = lane % 32 < 16

    far_cosine, far_sine = far_table[0:1, :], far_table[1:2, :]
    cosine = far_cosine * near_table[0] - far_sine * near_table[1]
    sine = far_sine * near_table[0] + far_cosine * near_table[1]
    sine = jnp.where(former, -sine, sine)

    def rotated(flat):
        floats = flat.astype(BF16).astype(F32)
        swapped = jnp.where(former, pltpu.roll(floats, 112, 1), pltpu.roll(floats, 16, 1))
        return (floats * cosine + swapped * sine).astype(BF16).astype(F32)

    product = dot(scaled, w[0]) * inverse
    queries = rotated(product[:, :128])
    keys = rotated(product[:, 128:])
    product = dot(scaled, w[1]) * inverse
    values = product[:, :128].astype(BF16).astype(F32)
    mq[...] = product[:, 128:].astype(BF16)
    held[0, sp] = jnp.where(low, keys, pltpu.roll(values, 64, 1)).astype(BF16)
    held[1, sp] = jnp.where(low, pltpu.roll(keys, 64, 1), values).astype(BF16)
    def z_copy(chain, way, hop, dx):
        dz = 1 - hop if way == 0 else hop - 1
        ref = held.at[1 if isinstance(chain, int) and chain == 0 else 0, span_at(dz, dx)]
        return remote(ref, ref, z_send.at[chain, way, hop - 1], z_recv.at[chain, way, hop - 1],
                      nexts[way], tp)

    def x_copy(number, kind, ring, dz):
        if kind < 2:
            ref = held.at[ring, span_at(dz, 0)]
        else:
            ref = held.at[ring, span_at(dz, 3 if kind == 2 else 1),
                          pl.ds((kind - 2) * half_rows, half_rows), :]
        return remote(ref, ref, x_send.at[number, kind], x_recv.at[number, kind],
                      nexts[2 + kind % 2], tp)

    for way in range(2):
        z_copy(0, way, 1, 0).start()
        x_copy(5, way, 0, 0).start()
    for way in range(2):
        z_copy(1, way, 1, 0).start()
        x_copy(0, way, 1, 0).start()

    for head in range(2):
        turned = queries if head == 0 else pltpu.roll(queries, 64, 1)
        for side in range(2):
            inside = (lane >= DD * side) & (lane < DD * side + DD)
            qs[head, side * rows:(side + 1) * rows, :] = jnp.where(inside, turned, 0.0).astype(BF16)
    product = dot(scaled, w[2]) * inverse
    mk[...] = product[:, :128].astype(BF16)
    mv[...] = product[:, 128:].astype(BF16)
    inverse_row = jnp.transpose(jnp.broadcast_to(inverse, (rows, 128)))[0:1, :]
    gate_in = dot_t(wig[...], scaled) * inverse_row
    forget = dot_t(wfg[...], scaled) * inverse_row

    def log_sigmoid(a):
        return jnp.minimum(a, 0.0) - jnp.log1p(jnp.exp(-jnp.abs(a)))

    def per_head(parts):
        return jnp.where(low, parts[0], parts[1])

    first_row = lax.broadcasted_iota(jnp.int32, (2, rows), 0) == 0
    log_forget = log_sigmoid(forget + jnp.where(first_row, bias[0], bias[1])) + decay[...]
    before_or_at = (lax.broadcasted_iota(jnp.int32, (rows, rows), 1)
                    <= lax.broadcasted_iota(jnp.int32, (rows, rows), 0))
    triangle = jnp.where(before_or_at, 1.0, 0.0).astype(BF16)
    high, middle, small = thirds(log_forget)
    cumulative = dot_t(high, triangle) + dot_t(middle, triangle) + dot_t(small, triangle)
    gate_rows[...] = gate_in - cumulative
    upper_rows = lax.broadcasted_iota(jnp.int32, (128, rows), 0) < HEAD

    def columns(pair):
        return jnp.transpose(jnp.where(upper_rows, pair[0:1, :], pair[1:2, :]))

    gates[0] = columns(cumulative)
    gates[1] = columns(gate_rows[...])
    span_decay = gates[0, rows - 1:rows, :]
    toward_end = span_decay + gates[1]
    span_top = jnp.max(toward_end, axis=0, keepdims=True)
    end_weights = jnp.exp(toward_end - span_top)
    key_floats = mk[...].astype(F32) * 0.125
    weighted = jnp.transpose(end_weights * mv[...].astype(F32))
    high, small = halves(weighted)
    keys_exact = key_floats.astype(BF16)
    outer = dot(high, keys_exact) + dot(small, keys_exact)
    row = lax.broadcasted_iota(jnp.int32, (8, 128), 0)

    def tail(normal, stable, decays):
        return jnp.where(row == 0, normal, jnp.where(row == 1, stable, decays))

    low_square = low[:HEAD]
    st_out[0, 0:HEAD, :] = jnp.where(low_square, outer[:HEAD], outer[HEAD:])
    st_out[0, HEAD:HEAD + 8, :] = tail(
        jnp.sum(end_weights * key_floats, axis=0, keepdims=True), span_top, span_decay)
    for kind in range(2):
        st_before[kind, 0:HEAD, :] = jnp.zeros((HEAD, 128), F32)
        st_before[kind, HEAD:HEAD + 8, :] = tail(0.0, NEGATIVE, 0.0) + jnp.zeros((8, 128), F32)

    def rise(number):
        return jnp.where(number == 2, 1, jnp.where(number == 3, 2, 4))

    def scan_copy(number):
        beside = jnp.where(number == 0, across_x + 1 - 2 * (across_x % 2), (across_x + 2) % 4)
        target = jnp.where(number < 2, 4 * z + beside, 4 * ((z + rise(number)) % 8) + across_x)
        return remote(st_out.at[number], st_in.at[number], scan_send.at[number],
                      scan_recv.at[number], target, tp)

    def joined(earlier, later):
        old, new = earlier[1], later[1]
        decays, stable, later_stable = new[2:3], old[1:2], new[1:2]
        highest = jnp.maximum(decays + stable, later_stable)
        first = jnp.exp(decays + stable - highest)
        second = jnp.exp(later_stable - highest)
        return (first * earlier[0] + second * later[0],
                tail(first * old[0:1] + second * new[0:1], highest, old[2:3] + decays))

    scale = DD ** (-0.5) * LOG2E

    def visit(ring, position, mask=None, other=None):
        block = held[ring, position]
        if other is not None:
            block = jnp.concatenate([block, held[ring, other]], axis=0)
        some = lax.broadcasted_iota(jnp.int32, block.shape, 1) < HEAD
        extended = jnp.where(some, jnp.ones_like(block), block)
        scores = dot_t(qs[ring], block)
        if mask is not None:
            scores = jnp.where(mask, scores, NEGATIVE)
            highest = jnp.broadcast_to(jnp.max(scores, axis=1, keepdims=True), (2 * rows, 128))
        else:
            old = top[ring]
            highest = jnp.maximum(old, jnp.max(scores, axis=1, keepdims=True))
        shift = highest * scale
        weights = jnp.exp2(scores * scale - jnp.concatenate([shift] * (block.shape[0] // 128), axis=1))
        product = dot(weights.astype(BF16), extended)
        if mask is not None:
            acc[ring] = product
        else:
            acc[ring] = acc[ring] * jnp.exp2((old - highest) * scale) + product
        top[ring] = highest

    causal = jnp.concatenate([before_or_at, before_or_at], axis=0)
    visit(0, sp, causal)
    scan_copy(0).start()
    x_copy(5, 0, 0, 0).wait_recv()
    x_copy(5, 2, 0, 0).start()
    for way in range(2):
        z_copy(2, way, 1, 3).start()
    x_copy(5, 1, 0, 0).wait_recv()
    x_copy(5, 3, 0, 0).start()
    for way in range(2):
        z_copy(3, way, 1, 1).start()
    visit(1, sp, causal)

    def local_memory():
        sums, tops, totals = [], [], []
        for head in range(2):
            inside = low if head == 0 else ~low
            gap = gates[0, :, HEAD * head:HEAD * head + 1] + gate_rows[head:head + 1, :]
            gap = jnp.where(before_or_at, gap, NEGATIVE)
            highest = jnp.max(gap, axis=1, keepdims=True)
            within = jnp.exp(gap - highest)
            mine = jnp.where(inside, mq[...].astype(F32), 0.0).astype(BF16)
            scores = within * (dot_t(mine, mk[...]) * 0.125)
            high, small = halves(scores)
            sums.append(dot(high, mv[...]) + dot(small, mv[...]))
            totals.append(jnp.sum(scores, axis=1, keepdims=True))
            tops.append(highest)
        num_local[0] = per_head(sums)
        num_local[1] = per_head(totals) + jnp.zeros((rows, 128), F32)
        log_local[...] = per_head(tops) + jnp.zeros((rows, 128), F32)

    def scan_round(number):
        scan_copy(number).wait_recv()
        memory = st_in[number, 0:HEAD, :]
        ending = st_in[number, HEAD:HEAD + 8, :]
        in_row = number < 2
        later_half = jnp.where(number == 0, across_x % 2, across_x // 2)
        earlier = jnp.where(in_row, later_half, jnp.where(z >= rise(number), 1, 0)) > 0
        kind = jnp.where(in_row, 0, 1)

        @pl.when(earlier)
        def _():
            done = joined((memory, ending),
                          (st_before[kind, 0:HEAD, :], st_before[kind, HEAD:HEAD + 8, :]))
            st_before[kind, 0:HEAD, :] = done[0]
            st_before[kind, HEAD:HEAD + 8, :] = done[1]

        @pl.when(number < ROUNDS - 1)
        def _():
            mine = (st_out[number, 0:HEAD, :], st_out[number, HEAD:HEAD + 8, :])
            after = joined((memory, ending), mine)
            ahead = joined(mine, (memory, ending))
            for place, (one, two, same) in enumerate(zip(after, ahead, mine)):
                merged = jnp.where(earlier, one, jnp.where(in_row, two, same))
                st_out[number + 1, HEAD * place:HEAD + 8 * place, :] = merged

    def attend(ring, pair):
        spans = [span_at(dz, dx) for dz, dx, _ in pair]
        counts = [valid & (span < sp) for span, (_, _, valid) in zip(spans, pair)]

        @pl.when(counts[0] & counts[1])
        def _():
            visit(ring, spans[0], other=spans[1])

        @pl.when(counts[0] != counts[1])
        def _():
            visit(ring, jnp.where(counts[0], spans[0], spans[1]))

    def attend_one(ring, dz, dx, valid):
        origin = span_at(dz, dx)

        @pl.when(valid & (origin < sp))
        def _():
            visit(ring, origin)

    def iteration(i, unused):
        pair, hop = i % 2, i // 2 + 1

        @pl.when((i >= 1) & (i < ROUNDS))
        def _():
            scan_copy(i).start()

        def own_chain(way):
            last = 4 - way

            @pl.when(i < last)
            def _():
                z_copy(0, way, i + 1, 0).wait_recv()

                @pl.when(i < last - 1)
                def _():
                    z_copy(0, way, i + 2, 0).start()

                for kind in range(2):
                    x_copy(5 * way + i + 1, kind, 1, (2 * way - 1) * (i + 1)).start()

        own_chain(0)
        own_chain(1)
        attend(1, ((-i - 1, 0, i < 4), (i + 1, 0, i < 3)))

        def x_arrival(rows_way, kind):
            valid = (i <= 4) if rows_way == 0 else (i >= 1) & (i <= 3)

            @pl.when(valid)
            def _():
                dz = (2 * rows_way - 1) * i
                x_copy(5 * rows_way + i, kind, 1, dz).wait_recv()
                x_copy(5 * rows_way + i, kind + 2, 1, dz).start()

        def x_attend(rows_way):
            j = i - X_LAG
            valid = (j >= 0) & (j <= 4) if rows_way == 0 else (j >= 1) & (j <= 3)
            dz = (2 * rows_way - 1) * j
            attend(1, ((dz, 3, valid), (dz, 1, valid)))

        x_arrival(0, 0)
        x_arrival(0, 1)
        x_attend(0)

        @pl.when(i == 0)
        def _():
            x_copy(5, 2, 0, 0).wait_recv()
            x_copy(5, 3, 0, 0).wait_recv()
            for way in range(2):
                z_copy(4, way, 1, 2).start()

        def chain(number, way, dx, last):
            @pl.when(hop <= last)
            def _():
                z_copy(number, way, hop, dx).wait_recv()

                @pl.when(hop < last)
                def _():
                    z_copy(number, way, hop + 1, dx).start()

        first = 1 + 2 * pair

        chain(first, 0, pair, 4)
        chain(first, 1, pair, 3)
        attend(0, ((-hop, pair, hop <= 4), (hop, pair, hop <= 3)))
        x_arrival(1, 0)
        x_arrival(1, 1)
        x_attend(1)
        chain(first + 1, 0, 3 - pair, 3)
        chain(first + 1, 1, 3 - pair, 4)
        attend(0, ((-hop, 3 - pair, hop <= 3), (hop, 3 - pair, hop <= 4)))

        def relayed(rows_way):
            j = i - 1
            valid = (j >= 0) & (j <= 4) if rows_way == 0 else (j >= 1) & (j <= 3)

            @pl.when(valid)
            def _():
                for kind in (2, 3):
                    x_copy(5 * rows_way + j, kind, 1, (2 * rows_way - 1) * j).wait_recv()

        relayed(0)
        relayed(1)
        j = i - 1 - RELAY_LAG
        attend(1, ((-j, 2, (j >= 0) & (j <= 4)), (j, 2, (j >= 1) & (j <= 3))))
        attend_one(0, 0, 3 - i, i < 3)

        @pl.when(i == 0)
        def _():
            local_memory()

        @pl.when(i < ROUNDS)
        def _():
            scan_round(i)

        return unused

    lax.fori_loop(0, 8, iteration, 0)
    for number, lasts in enumerate(((4, 3), (4, 3), (3, 4), (4, 3), (3, 4))):
        for way, last in enumerate(lasts):
            for hop in range(1, last + 1):
                z_copy(number, way, hop, 0).wait_send()
    for number in range(9):
        for kind in range(4):
            x_copy(number, kind, 1, 0).wait_send()
    for number in range(ROUNDS):
        scan_copy(number).wait_send()

    rooted = []
    for head in range(2):
        sides = []
        for side in range(2):
            part = acc[head, side * rows:(side + 1) * rows, :]
            sides.append(part / pltpu.roll(part, 64, 1))
        difference = sides[0] - lambdas[head] * sides[1]
        squared = jnp.where(low, 0.0, difference * difference)
        mean = jnp.sum(squared, axis=1, keepdims=True) * (1.0 / HEAD)
        rooted.append(difference * lax.rsqrt(mean + EPSILON))
    cat[:, 0:128] = (jnp.where(low, pltpu.roll(rooted[0], 64, 1), rooted[1])
                     * jnp.concatenate([head_gain[...]] * 2, axis=1)).astype(BF16)

    start_memory = jnp.zeros((HEAD, 128), F32)
    start_tail = jnp.zeros((8, 128), F32)
    entered = (start_memory, start_tail)
    for kind in (1, 0):
        entered = joined(entered, (st_before[kind, 0:HEAD, :], st_before[kind, HEAD:HEAD + 8, :]))
    memory_in, normal_in, stable_in = entered[0], entered[1][0:1], entered[1][1:2]
    spread = jnp.concatenate(
        [jnp.where(low_square, memory_in, 0.0), jnp.where(low_square, 0.0, memory_in)], axis=0)
    spread_normal = jnp.concatenate(
        [jnp.where(low_square, normal_in, 0.0), jnp.where(low_square, 0.0, normal_in)], axis=0)
    carried_log = gates[0] + stable_in
    row_top = jnp.maximum(carried_log, log_local[...])
    outside = jnp.exp(carried_log - row_top)
    inside = jnp.exp(log_local[...] - row_top)
    high, small = halves(spread)
    numerator = outside * (dot_t(mq[...], high) + dot_t(mq[...], small)) + inside * num_local[0]
    high, small = halves(spread_normal)
    denominator = outside * (dot_t(mq[...], high) + dot_t(mq[...], small)) + inside * num_local[1]
    cat[:, 128:256] = (numerator / jnp.maximum(jnp.abs(denominator), 1.0)).astype(BF16)

    for load in out_loads:
        load.wait()
    both = cat[...]

    def share(seat):
        return dot(both, wo[seat]).astype(BF16)

    offsets = (2, 1, 3, 0)
    pairs = []
    for number, offset in enumerate(offsets):
        to_partner[number] = share(2 * ((y + offset) % 4) + 1 - c)
        pairs.append(remote(to_partner.at[number], from_partner.at[number], pair_send.at[number],
                            pair_recv.at[number], sp, partner))
        pairs[number].start()

    def summed(number):
        own = share(2 * ((y + offsets[number]) % 4) + c).astype(F32)
        pairs[number].wait_recv()
        return own + from_partner[number].astype(F32)

    def shift(number, seat, part=None):
        if part is None:
            source, target = to_ring.at[number], from_ring.at[number]
        else:
            span = pl.ds(part * quarter, quarter)
            source, target = to_ring.at[number, span, :], from_ring.at[number, span, :]
        lane_of = part or 0
        return remote(source, target, sum_send.at[number, lane_of], sum_recv.at[number, lane_of],
                      sp, seat)

    across_right = [shift(0, right, part) for part in range(2)]
    across_left = [shift(1, left, part) for part in range(2)]
    along_right, along_left = shift(2, right), shift(4, left)
    added_right = [shift(3, right, part) for part in range(2)]
    added_left = [shift(5, left, part) for part in range(2)]
    total = summed(0)
    to_ring[0] = total[:half_rows].astype(BF16)
    to_ring[1] = total[half_rows:].astype(BF16)
    for part in range(2):
        across_right[part].start()
        across_left[part].start()
    total = summed(1)
    to_ring[2] = total[half_rows:].astype(BF16)
    along_right.start()
    rest = total[:half_rows]
    total = summed(2)
    to_ring[4] = total[:half_rows].astype(BF16)
    along_left.start()
    other = total[half_rows:]
    total = summed(3)
    for part in range(2):
        span = slice(part * quarter, (part + 1) * quarter)
        across_right[part].wait_recv()
        to_ring[3, span, :] = (rest[span] + from_ring[0, span, :].astype(F32)).astype(BF16)
        added_right[part].start()
        across_left[part].wait_recv()
        to_ring[5, span, :] = (other[span] + from_ring[1, span, :].astype(F32)).astype(BF16)
        added_left[part].start()
    along_right.wait_recv()
    along_left.wait_recv()
    lower = total[half_rows:] + from_ring[2].astype(F32)
    upper = total[:half_rows] + from_ring[4].astype(F32)
    for part in range(2):
        span = slice(part * quarter, (part + 1) * quarter)
        added_right[part].wait_recv()
        out[span, :] = (upper[span] + from_ring[3, span, :].astype(F32)).astype(BF16)
        added_left[part].wait_recv()
        out[half_rows + part * quarter:half_rows + (part + 1) * quarter, :] = (
            lower[span] + from_ring[5, span, :].astype(F32)).astype(BF16)
    shifts = across_right + across_left + added_right + added_left + [along_right, along_left]
    for copy in pairs + shifts:
        copy.wait_send()


def per_device(
    inputs, norm_gain, query_weight, key_weight, value_weight, memory_query_weight,
    memory_key_weight, memory_value_weight, input_gate_weight, forget_gate_weight, forget_bias,
    decay_shift, lambdas, head_gain, out_weight_attention, out_weight_memory,
):
    rows, columns = inputs.shape
    middle = DD // 2
    inverse = 1.0 / ROTARY_BASE ** (np.arange(middle) / middle)
    near = np.tile(np.arange(rows)[:, None] * inverse[None, :], (1, 8))
    far = np.tile((np.arange(SPANS) * rows)[:, None] * inverse[None, :], (1, 8))
    near = jnp.asarray(np.stack([np.cos(near), np.sin(near)]), F32)
    far = jnp.asarray(np.stack([np.cos(far), np.sin(far)], axis=1), F32)
    vmem = pl.BlockSpec(memory_space=pltpu.VMEM)
    anywhere = pl.BlockSpec(memory_space=pl.ANY)
    half = rows // 2
    scratch = [
        pltpu.VMEM((8, 1, columns), F32),
        pltpu.VMEM((2, rows, 128), F32),
        pltpu.VMEM((2, 128), F32),
        pltpu.VMEM((2, 2048), BF16),
        pltpu.VMEM((2, 2048), BF16),
        pltpu.SMEM((2,), F32),
        pltpu.VMEM((2, rows), F32),
        pltpu.SMEM((2,), F32),
        pltpu.VMEM((1, HEAD), F32),
        pltpu.VMEM((8, rows, columns), BF16),
        pltpu.VMEM((8, rows, columns), BF16),
        pltpu.VMEM((rows, columns), F32),
        pltpu.VMEM((3, 2048, 256), BF16),
        pltpu.VMEM((8, 256, 256), BF16),
        pltpu.VMEM((2, SPANS, rows, 128), BF16),
        pltpu.VMEM((2, 2 * rows, 128), BF16),
        pltpu.VMEM((rows, 128), BF16),
        pltpu.VMEM((rows, 128), BF16),
        pltpu.VMEM((rows, 128), BF16),
        pltpu.VMEM((2, rows, 128), F32),
        pltpu.VMEM((2, rows), F32),
        pltpu.VMEM((2, 2 * rows, 128), F32),
        pltpu.VMEM((2, 2 * rows, 128), F32),
        pltpu.VMEM((ROUNDS, HEAD + 8, 128), F32),
        pltpu.VMEM((ROUNDS, HEAD + 8, 128), F32),
        pltpu.VMEM((2, HEAD + 8, 128), F32),
        pltpu.VMEM((2, rows, 128), F32),
        pltpu.VMEM((rows, 128), F32),
        pltpu.VMEM((rows, 256), BF16),
        pltpu.VMEM((4, rows, 256), BF16),
        pltpu.VMEM((4, rows, 256), BF16),
        pltpu.VMEM((6, half, 256), BF16),
        pltpu.VMEM((6, half, 256), BF16),
        pltpu.SemaphoreType.DMA((9,)),
        pltpu.SemaphoreType.DMA((25,)),
        pltpu.SemaphoreType.DMA((13, 2)),
        pltpu.SemaphoreType.DMA((13, 2)),
        pltpu.SemaphoreType.DMA((5, 2, 4)),
        pltpu.SemaphoreType.DMA((5, 2, 4)),
        pltpu.SemaphoreType.DMA((10, 4)),
        pltpu.SemaphoreType.DMA((10, 4)),
        pltpu.SemaphoreType.DMA((ROUNDS,)),
        pltpu.SemaphoreType.DMA((ROUNDS,)),
        pltpu.SemaphoreType.DMA((4,)),
        pltpu.SemaphoreType.DMA((4,)),
        pltpu.SemaphoreType.DMA((6, 2)),
        pltpu.SemaphoreType.DMA((6, 2)),
    ]
    return pl.pallas_call(
        layer_kernel,
        out_shape=jax.ShapeDtypeStruct((rows, columns), BF16),
        in_specs=[anywhere] * 18,
        out_specs=vmem,
        scratch_shapes=scratch,
        compiler_params=pltpu.CompilerParams(
            collective_id=0, has_side_effects=True, vmem_limit_bytes=60 * 1024 * 1024),
        name="layer",
    )(
        inputs, norm_gain.reshape(8, 1, 256), near, far, query_weight, key_weight, value_weight,
        memory_query_weight, memory_key_weight, memory_value_weight, input_gate_weight.T,
        forget_gate_weight.T, forget_bias, decay_shift.T, lambdas, head_gain.reshape(1, HEAD),
        out_weight_attention, out_weight_memory,
    )


def solution(mesh):
    split = P(None, "tp")
    placed = (
        P("sp", "tp"), P(), split, split, split, split, split, split, split, split,
        P("tp"), P("sp", "tp"), P("tp"), P(), P("tp", None), P("tp", None),
    )
    return jax.shard_map(
        per_device, mesh=mesh, in_specs=placed, out_specs=P("sp", "tp"), check_vma=False)
```

```python
import jax
import numpy as np
import jax.numpy as jnp
from jax import lax
from jax.experimental import pallas as pl
from jax.experimental.pallas import tpu as pltpu
from jax.sharding import PartitionSpec as P

HEAD = 64
DD = 32
EPSILON = 1e-06
ROTARY_BASE = 10000.0
NEGATIVE = -1e30
LOG2E = 1.4426950408889634
SPANS = 32
ROUNDS = 5
X_LAG = 0
RELAY_LAG = 0
MESH = pl.DeviceIdType.MESH
F32 = jnp.float32
BF16 = jnp.bfloat16


def dot(a, b):
    return jnp.dot(a, b, preferred_element_type=F32)


def dot_t(a, b):
    return lax.dot_general(a, b, (((1,), (1,)), ((), ())), preferred_element_type=F32)


def halves(a):
    high = a.astype(BF16)
    return high, (a - high.astype(F32)).astype(BF16)


def thirds(a):
    high = a.astype(BF16)
    rest = a - high.astype(F32)
    middle = rest.astype(BF16)
    return high, middle, (rest - middle.astype(F32)).astype(BF16)


def layer_kernel(
    x, gain_in, near_in, far_in, wq, wk, wv, wmq, wmk, wmv, wig_in, wfg_in, bias_in, decay_in,
    lambdas_in, head_gain_in, woa, wom, out,
    gain, near_table, far_table, wig, wfg, bias, decay, lambdas, head_gain,
    xg, xs, squares, w, wo, held, qs, mq, mk, mv, gates, gate_rows, acc, top, st_in, st_out, st_before,
    num_local, log_local, cat, to_partner, from_partner, to_ring, from_ring,
    small_sem, load_sem, gather_send, gather_recv, z_send, z_recv, x_send, x_recv, scan_send, scan_recv,
    pair_send, pair_recv, sum_send, sum_recv,
):
    rows = x.shape[0]
    half_rows = rows // 2
    sp = lax.axis_index("sp")
    tp = lax.axis_index("tp")
    y, c = tp // 2, tp % 2
    right = 2 * ((y + 1) % 4) + c
    left = 2 * ((y + 3) % 4) + c
    across = 2 * ((y + 2) % 4) + c
    partner = 2 * y + 1 - c
    z, across_x = sp // 4, sp % 4
    above, below = 4 * ((z + 1) % 8) + across_x, 4 * ((z + 7) % 8) + across_x
    nexts = [above, below, 4 * z + (across_x + 1) % 4, 4 * z + (across_x + 3) % 4]

    def span_at(dz, dx):
        return 4 * ((z + dz + 16) % 8) + (across_x + dx) % 4

    def remote(src, dst, send, recv, span, seat):
        return pltpu.make_async_remote_copy(
            src_ref=src, dst_ref=dst, send_sem=send, recv_sem=recv,
            device_id=(span, seat), device_id_type=MESH)

    barrier = pltpu.get_barrier_semaphore()
    greeted = [(sp, right), (sp, left), (sp, partner)] + [(span, tp) for span in nexts]
    for span, seat in greeted:
        pl.semaphore_signal(barrier, inc=1, device_id=(span, seat), device_id_type=MESH)

    own_load = pltpu.make_async_copy(x, xg.at[tp], load_sem.at[0])
    own_load.start()
    loads = []
    for number, (weight, tile, at) in enumerate(
            ((wq, 0, 0), (wk, 0, 128), (wv, 1, 0), (wmq, 1, 128), (wmk, 2, 0), (wmv, 2, 128))):
        loads.append(pltpu.make_async_copy(
            weight, w.at[tile, :, pl.ds(at, 128)], load_sem.at[1 + number]))
    small_loads = {}
    for number, (source, target) in enumerate((
            (gain_in, gain), (near_in, near_table), (far_in.at[sp], far_table), (wig_in, wig),
            (wfg_in, wfg), (bias_in, bias), (decay_in, decay), (lambdas_in, lambdas),
            (head_gain_in, head_gain))):
        small_loads[number] = pltpu.make_async_copy(source, target, small_sem.at[number])
        small_loads[number].start()
    for load in loads:
        load.start()
    out_loads = []
    for j in range(8):
        for part, weight in enumerate((woa, wom)):
            out_loads.append(pltpu.make_async_copy(
                weight.at[:, pl.ds(256 * j, 256)], wo.at[j, pl.ds(128 * part, 128), :],
                load_sem.at[9 + 2 * j + part]))
    for load in out_loads:
        load.start()

    quarter = half_rows // 2

    def piece(seat, half, part=None):
        if part is None:
            return xg.at[seat, pl.ds(half * half_rows, half_rows), :]
        return xg.at[seat, pl.ds(half * half_rows + part * quarter, quarter), :]

    def gather(number, seat, goal, half=None):
        if half is None:
            ref = xg.at[seat]
            return [remote(ref, ref, gather_send.at[number, 0], gather_recv.at[number, 0], sp, goal)]
        if number in (1, 3, 6, 8, 9, 10):
            ref = piece(seat, half)
            return [remote(ref, ref, gather_send.at[number, 0], gather_recv.at[number, 0], sp, goal)]
        refs = [piece(seat, half, part) for part in range(2)]
        return [remote(ref, ref, gather_send.at[number, part], gather_recv.at[number, part], sp, goal)
                for part, ref in enumerate(refs)]

    sends = {
        0: gather(0, tp, right, 0),
        1: gather(1, tp, right, 1),
        2: gather(2, tp, left, 1),
        3: gather(3, tp, left, 0),
        4: gather(4, tp, partner),
        5: gather(5, left, right, 0),
        6: gather(6, left, partner, 0),
        7: gather(7, right, left, 1),
        8: gather(8, right, partner, 1),
        9: gather(9, left, partner, 1),
        10: gather(10, right, partner, 0),
        11: gather(11, across, partner, 0),
        12: gather(12, across, partner, 1),
    }
    own_load.wait()
    pl.semaphore_wait(barrier, len(greeted))
    for part in range(2):
        sends[0][part].start()
        sends[2][part].start()
    for number in (1, 3, 4):
        sends[number][0].start()

    def absorb(seat):
        block = xg[seat].astype(F32)
        squares[...] += block * block
        xs[seat] = (block * gain[seat]).astype(BF16)

    squares[...] = jnp.zeros_like(squares)
    small_loads[0].wait()
    absorb(tp)
    for part in range(2):
        sends[0][part].wait_recv()
        sends[5][part].start()
        sends[2][part].wait_recv()
        sends[7][part].start()
    sends[6][0].start()
    sends[8][0].start()
    sends[4][0].wait_recv()
    absorb(partner)
    sends[1][0].wait_recv()
    sends[9][0].start()
    sends[3][0].wait_recv()
    sends[10][0].start()
    absorb(left)
    absorb(right)
    for part in range(2):
        sends[5][part].wait_recv()
        sends[11][part].start()
        sends[7][part].wait_recv()
        sends[12][part].start()
    for number in (6, 8, 9, 10):
        sends[number][0].wait_recv()
    absorb(2 * ((y + 1) % 4) + 1 - c)
    absorb(2 * ((y + 3) % 4) + 1 - c)
    absorb(across)
    for part in range(2):
        sends[11][part].wait_recv()
        sends[12][part].wait_recv()
    absorb(2 * ((y + 2) % 4) + 1 - c)
    for number in range(13):
        for copy in sends[number]:
            copy.wait_send()
    for load in loads + [small_loads[number] for number in range(1, 9)]:
        load.wait()

    inverse = lax.rsqrt(
        jnp.sum(squares[...], axis=1, keepdims=True) * (1.0 / 2048.0) + EPSILON)
    scaled = jnp.concatenate([xs[j] for j in range(8)], axis=1)
    lane = lax.broadcasted_iota(jnp.int32, (rows, 128), 1)
    low = lane < HEAD
    former = lane % 32 < 16

    far_cosine, far_sine = far_table[0:1, :], far_table[1:2, :]
    cosine = far_cosine * near_table[0] - far_sine * near_table[1]
    sine = far_sine * near_table[0] + far_cosine * near_table[1]
    sine = jnp.where(former, -sine, sine)

    def rotated(flat):
        floats = flat.astype(BF16).astype(F32)
        swapped = jnp.where(former, pltpu.roll(floats, 112, 1), pltpu.roll(floats, 16, 1))
        return (floats * cosine + swapped * sine).astype(BF16).astype(F32)

    product = dot(scaled, w[0]) * inverse
    queries = rotated(product[:, :128])
    keys = rotated(product[:, 128:])
    product = dot(scaled, w[1]) * inverse
    values = product[:, :128].astype(BF16).astype(F32)
    mq[...] = product[:, 128:].astype(BF16)
    held[0, sp] = jnp.where(low, keys, pltpu.roll(values, 64, 1)).astype(BF16)
    held[1, sp] = jnp.where(low, pltpu.roll(keys, 64, 1), values).astype(BF16)
    def z_copy(chain, way, hop, dx):
        dz = 1 - hop if way == 0 else hop - 1
        ref = held.at[1 if isinstance(chain, int) and chain == 0 else 0, span_at(dz, dx)]
        return remote(ref, ref, z_send.at[chain, way, hop - 1], z_recv.at[chain, way, hop - 1],
                      nexts[way], tp)

    def x_copy(number, kind, ring, dz):
        if kind < 2:
            ref = held.at[ring, span_at(dz, 0)]
        else:
            ref = held.at[ring, span_at(dz, 3 if kind == 2 else 1),
                          pl.ds((kind - 2) * half_rows, half_rows), :]
        return remote(ref, ref, x_send.at[number, kind], x_recv.at[number, kind],
                      nexts[2 + kind % 2], tp)

    for way in range(2):
        z_copy(0, way, 1, 0).start()
        x_copy(5, way, 0, 0).start()
    for way in range(2):
        z_copy(1, way, 1, 0).start()
        x_copy(0, way, 1, 0).start()

    for head in range(2):
        turned = queries if head == 0 else pltpu.roll(queries, 64, 1)
        for side in range(2):
            inside = (lane >= DD * side) & (lane < DD * side + DD)
            qs[head, side * rows:(side + 1) * rows, :] = jnp.where(inside, turned, 0.0).astype(BF16)
    before_or_at = (lax.broadcasted_iota(jnp.int32, (rows, rows), 1)
                    <= lax.broadcasted_iota(jnp.int32, (rows, rows), 0))

    scale = DD ** (-0.5) * LOG2E

    def visit(ring, position, mask=None, other=None):
        block = held[ring, position]
        if other is not None:
            block = jnp.concatenate([block, held[ring, other]], axis=0)
        some = lax.broadcasted_iota(jnp.int32, block.shape, 1) < HEAD
        extended = jnp.where(some, jnp.ones_like(block), block)
        scores = dot_t(qs[ring], block)
        if mask is not None:
            scores = jnp.where(mask, scores, NEGATIVE)
            highest = jnp.broadcast_to(jnp.max(scores, axis=1, keepdims=True), (2 * rows, 128))
        else:
            old = top[ring]
            highest = jnp.maximum(old, jnp.max(scores, axis=1, keepdims=True))
        shift = highest * scale
        weights = jnp.exp2(scores * scale - jnp.concatenate([shift] * (block.shape[0] // 128), axis=1))
        product = dot(weights.astype(BF16), extended)
        if mask is not None:
            acc[ring] = product
        else:
            acc[ring] = acc[ring] * jnp.exp2((old - highest) * scale) + product
        top[ring] = highest

    causal = jnp.concatenate([before_or_at, before_or_at], axis=0)
    visit(0, sp, causal)
    visit(1, sp, causal)

    product = dot(scaled, w[2]) * inverse
    mk[...] = product[:, :128].astype(BF16)
    mv[...] = product[:, 128:].astype(BF16)
    inverse_row = jnp.transpose(jnp.broadcast_to(inverse, (rows, 128)))[0:1, :]
    gate_weights = jnp.concatenate([wig[...].astype(F32), wfg[...].astype(F32)], axis=0)
    both_gates = dot_t(gate_weights.astype(BF16), scaled) * inverse_row
    gate_in, forget = both_gates[0:2], both_gates[2:4]

    def log_sigmoid(a):
        return jnp.minimum(a, 0.0) - jnp.log1p(jnp.exp(-jnp.abs(a)))

    def per_head(parts):
        return jnp.where(low, parts[0], parts[1])

    first_row = lax.broadcasted_iota(jnp.int32, (2, rows), 0) == 0
    log_forget = log_sigmoid(forget + jnp.where(first_row, bias[0], bias[1])) + decay[...]
    triangle = jnp.where(before_or_at, 1.0, 0.0).astype(BF16)
    high, middle, small = thirds(log_forget)
    cumulative = dot_t(high, triangle) + dot_t(middle, triangle) + dot_t(small, triangle)
    gate_rows[...] = gate_in - cumulative
    upper_rows = lax.broadcasted_iota(jnp.int32, (128, rows), 0) < HEAD

    def columns(pair):
        return jnp.transpose(jnp.where(upper_rows, pair[0:1, :], pair[1:2, :]))

    gates[0] = columns(cumulative)
    gates[1] = columns(gate_rows[...])
    x_copy(5, 0, 0, 0).wait_recv()
    x_copy(5, 2, 0, 0).start()
    for way in range(2):
        z_copy(2, way, 1, 3).start()
    x_copy(5, 1, 0, 0).wait_recv()
    x_copy(5, 3, 0, 0).start()
    for way in range(2):
        z_copy(3, way, 1, 1).start()
    span_decay = gates[0, rows - 1:rows, :]
    toward_end = span_decay + gates[1]
    span_top = jnp.max(toward_end, axis=0, keepdims=True)
    end_weights = jnp.exp(toward_end - span_top)
    key_floats = mk[...].astype(F32) * 0.125
    weighted = jnp.transpose(end_weights * mv[...].astype(F32))
    high, small = halves(weighted)
    keys_exact = key_floats.astype(BF16)
    outer = dot(high, keys_exact) + dot(small, keys_exact)
    row = lax.broadcasted_iota(jnp.int32, (8, 128), 0)

    def tail(normal, stable, decays):
        return jnp.where(row == 0, normal, jnp.where(row == 1, stable, decays))

    low_square = low[:HEAD]
    st_out[0, 0:HEAD, :] = jnp.where(low_square, outer[:HEAD], outer[HEAD:])
    st_out[0, HEAD:HEAD + 8, :] = tail(
        jnp.sum(end_weights * key_floats, axis=0, keepdims=True), span_top, span_decay)
    for kind in range(2):
        st_before[kind, 0:HEAD, :] = jnp.zeros((HEAD, 128), F32)
        st_before[kind, HEAD:HEAD + 8, :] = tail(0.0, NEGATIVE, 0.0) + jnp.zeros((8, 128), F32)

    def rise(number):
        return jnp.where(number == 2, 1, jnp.where(number == 3, 2, 4))

    def scan_copy(number):
        beside = jnp.where(number == 0, across_x + 1 - 2 * (across_x % 2), (across_x + 2) % 4)
        target = jnp.where(number < 2, 4 * z + beside, 4 * ((z + rise(number)) % 8) + across_x)
        return remote(st_out.at[number], st_in.at[number], scan_send.at[number],
                      scan_recv.at[number], target, tp)

    def joined(earlier, later):
        old, new = earlier[1], later[1]
        decays, stable, later_stable = new[2:3], old[1:2], new[1:2]
        highest = jnp.maximum(decays + stable, later_stable)
        first = jnp.exp(decays + stable - highest)
        second = jnp.exp(later_stable - highest)
        return (first * earlier[0] + second * later[0],
                tail(first * old[0:1] + second * new[0:1], highest, old[2:3] + decays))

    scan_copy(0).start()

    def local_memory():
        sums, tops, totals = [], [], []
        for head in range(2):
            inside = low if head == 0 else ~low
            gap = gates[0, :, HEAD * head:HEAD * head + 1] + gate_rows[head:head + 1, :]
            gap = jnp.where(before_or_at, gap, NEGATIVE)
            highest = jnp.max(gap, axis=1, keepdims=True)
            within = jnp.exp(gap - highest)
            mine = jnp.where(inside, mq[...].astype(F32), 0.0).astype(BF16)
            scores = within * (dot_t(mine, mk[...]) * 0.125)
            high, small = halves(scores)
            sums.append(dot(high, mv[...]) + dot(small, mv[...]))
            totals.append(jnp.sum(scores, axis=1, keepdims=True))
            tops.append(highest)
        num_local[0] = per_head(sums)
        num_local[1] = per_head(totals) + jnp.zeros((rows, 128), F32)
        log_local[...] = per_head(tops) + jnp.zeros((rows, 128), F32)

    def scan_round(number):
        scan_copy(number).wait_recv()
        memory = st_in[number, 0:HEAD, :]
        ending = st_in[number, HEAD:HEAD + 8, :]
        in_row = number < 2
        later_half = jnp.where(number == 0, across_x % 2, across_x // 2)
        earlier = jnp.where(in_row, later_half, jnp.where(z >= rise(number), 1, 0)) > 0
        kind = jnp.where(in_row, 0, 1)

        @pl.when(earlier)
        def _():
            done = joined((memory, ending),
                          (st_before[kind, 0:HEAD, :], st_before[kind, HEAD:HEAD + 8, :]))
            st_before[kind, 0:HEAD, :] = done[0]
            st_before[kind, HEAD:HEAD + 8, :] = done[1]

        @pl.when(number < ROUNDS - 1)
        def _():
            mine = (st_out[number, 0:HEAD, :], st_out[number, HEAD:HEAD + 8, :])
            after = joined((memory, ending), mine)
            ahead = joined(mine, (memory, ending))
            for place, (one, two, same) in enumerate(zip(after, ahead, mine)):
                merged = jnp.where(earlier, one, jnp.where(in_row, two, same))
                st_out[number + 1, HEAD * place:HEAD + 8 * place, :] = merged

    def attend(ring, pair):
        spans = [span_at(dz, dx) for dz, dx, _ in pair]
        counts = [valid & (span < sp) for span, (_, _, valid) in zip(spans, pair)]

        @pl.when(counts[0] & counts[1])
        def _():
            visit(ring, spans[0], other=spans[1])

        @pl.when(counts[0] != counts[1])
        def _():
            visit(ring, jnp.where(counts[0], spans[0], spans[1]))

    def attend_one(ring, dz, dx, valid):
        origin = span_at(dz, dx)

        @pl.when(valid & (origin < sp))
        def _():
            visit(ring, origin)

    def iteration(i, unused):
        pair, hop = i % 2, i // 2 + 1

        @pl.when((i >= 1) & (i < ROUNDS))
        def _():
            scan_copy(i).start()

        def own_chain(way):
            last = 4 - way

            @pl.when(i < last)
            def _():
                z_copy(0, way, i + 1, 0).wait_recv()

                @pl.when(i < last - 1)
                def _():
                    z_copy(0, way, i + 2, 0).start()

                for kind in range(2):
                    x_copy(5 * way + i + 1, kind, 1, (2 * way - 1) * (i + 1)).start()

        own_chain(0)
        own_chain(1)
        attend(1, ((-i - 1, 0, i < 4), (i + 1, 0, i < 3)))

        def x_arrival(rows_way, kind):
            valid = (i <= 4) if rows_way == 0 else (i >= 1) & (i <= 3)

            @pl.when(valid)
            def _():
                dz = (2 * rows_way - 1) * i
                x_copy(5 * rows_way + i, kind, 1, dz).wait_recv()
                x_copy(5 * rows_way + i, kind + 2, 1, dz).start()

        def x_attend(rows_way):
            j = i - X_LAG
            valid = (j >= 0) & (j <= 4) if rows_way == 0 else (j >= 1) & (j <= 3)
            dz = (2 * rows_way - 1) * j
            attend(1, ((dz, 3, valid), (dz, 1, valid)))

        x_arrival(0, 0)
        x_arrival(0, 1)
        x_attend(0)

        @pl.when(i == 0)
        def _():
            x_copy(5, 2, 0, 0).wait_recv()
            x_copy(5, 3, 0, 0).wait_recv()
            for way in range(2):
                z_copy(4, way, 1, 2).start()

        def chain(number, way, dx, last):
            @pl.when(hop <= last)
            def _():
                z_copy(number, way, hop, dx).wait_recv()

                @pl.when(hop < last)
                def _():
                    z_copy(number, way, hop + 1, dx).start()

        first = 1 + 2 * pair

        chain(first, 0, pair, 4)
        chain(first, 1, pair, 3)
        attend(0, ((-hop, pair, hop <= 4), (hop, pair, hop <= 3)))
        x_arrival(1, 0)
        x_arrival(1, 1)
        x_attend(1)
        chain(first + 1, 0, 3 - pair, 3)
        chain(first + 1, 1, 3 - pair, 4)
        attend(0, ((-hop, 3 - pair, hop <= 3), (hop, 3 - pair, hop <= 4)))

        def relayed(rows_way):
            j = i - 1
            valid = (j >= 0) & (j <= 4) if rows_way == 0 else (j >= 1) & (j <= 3)

            @pl.when(valid)
            def _():
                for kind in (2, 3):
                    x_copy(5 * rows_way + j, kind, 1, (2 * rows_way - 1) * j).wait_recv()

        relayed(0)
        relayed(1)
        j = i - 1 - RELAY_LAG
        attend(1, ((-j, 2, (j >= 0) & (j <= 4)), (j, 2, (j >= 1) & (j <= 3))))
        attend_one(0, 0, 3 - i, i < 3)

        @pl.when(i == 0)
        def _():
            local_memory()

        @pl.when(i < ROUNDS)
        def _():
            scan_round(i)

        return unused

    lax.fori_loop(0, 8, iteration, 0)
    for number, lasts in enumerate(((4, 3), (4, 3), (3, 4), (4, 3), (3, 4))):
        for way, last in enumerate(lasts):
            for hop in range(1, last + 1):
                z_copy(number, way, hop, 0).wait_send()
    for number in range(9):
        for kind in range(4):
            x_copy(number, kind, 1, 0).wait_send()
    for number in range(ROUNDS):
        scan_copy(number).wait_send()

    rooted = []
    for head in range(2):
        sides = []
        for side in range(2):
            part = acc[head, side * rows:(side + 1) * rows, :]
            sides.append(part / pltpu.roll(part, 64, 1))
        difference = sides[0] - lambdas[head] * sides[1]
        squared = jnp.where(low, 0.0, difference * difference)
        mean = jnp.sum(squared, axis=1, keepdims=True) * (1.0 / HEAD)
        rooted.append(difference * lax.rsqrt(mean + EPSILON))
    cat[:, 0:128] = (jnp.where(low, pltpu.roll(rooted[0], 64, 1), rooted[1])
                     * jnp.concatenate([head_gain[...]] * 2, axis=1)).astype(BF16)

    start_memory = jnp.zeros((HEAD, 128), F32)
    start_tail = jnp.zeros((8, 128), F32)
    entered = (start_memory, start_tail)
    for kind in (1, 0):
        entered = joined(entered, (st_before[kind, 0:HEAD, :], st_before[kind, HEAD:HEAD + 8, :]))
    memory_in, normal_in, stable_in = entered[0], entered[1][0:1], entered[1][1:2]
    spread = jnp.concatenate(
        [jnp.where(low_square, memory_in, 0.0), jnp.where(low_square, 0.0, memory_in)], axis=0)
    spread_normal = jnp.concatenate(
        [jnp.where(low_square, normal_in, 0.0), jnp.where(low_square, 0.0, normal_in)], axis=0)
    carried_log = gates[0] + stable_in
    row_top = jnp.maximum(carried_log, log_local[...])
    outside = jnp.exp(carried_log - row_top)
    inside = jnp.exp(log_local[...] - row_top)
    high, small = halves(spread)
    numerator = outside * (dot_t(mq[...], high) + dot_t(mq[...], small)) + inside * num_local[0]
    high, small = halves(spread_normal)
    denominator = outside * (dot_t(mq[...], high) + dot_t(mq[...], small)) + inside * num_local[1]
    cat[:, 128:256] = (numerator / jnp.maximum(jnp.abs(denominator), 1.0)).astype(BF16)

    for load in out_loads:
        load.wait()
    both = cat[...]

    def share(seat):
        return dot(both, wo[seat]).astype(BF16)

    offsets = (2, 1, 3, 0)
    pairs = []
    for number, offset in enumerate(offsets):
        to_partner[number] = share(2 * ((y + offset) % 4) + 1 - c)
        pairs.append(remote(to_partner.at[number], from_partner.at[number], pair_send.at[number],
                            pair_recv.at[number], sp, partner))
        pairs[number].start()

    def summed(number):
        own = share(2 * ((y + offsets[number]) % 4) + c).astype(F32)
        pairs[number].wait_recv()
        return own + from_partner[number].astype(F32)

    def shift(number, seat, part=None):
        if part is None:
            source, target = to_ring.at[number], from_ring.at[number]
        else:
            span = pl.ds(part * quarter, quarter)
            source, target = to_ring.at[number, span, :], from_ring.at[number, span, :]
        lane_of = part or 0
        return remote(source, target, sum_send.at[number, lane_of], sum_recv.at[number, lane_of],
                      sp, seat)

    across_right = [shift(0, right, part) for part in range(2)]
    across_left = [shift(1, left, part) for part in range(2)]
    along_right, along_left = shift(2, right), shift(4, left)
    added_right = [shift(3, right, part) for part in range(2)]
    added_left = [shift(5, left, part) for part in range(2)]
    total = summed(0)
    to_ring[0] = total[:half_rows].astype(BF16)
    to_ring[1] = total[half_rows:].astype(BF16)
    for part in range(2):
        across_right[part].start()
        across_left[part].start()
    total = summed(1)
    to_ring[2] = total[half_rows:].astype(BF16)
    along_right.start()
    rest = total[:half_rows]
    total = summed(2)
    to_ring[4] = total[:half_rows].astype(BF16)
    along_left.start()
    other = total[half_rows:]
    total = summed(3)
    for part in range(2):
        span = slice(part * quarter, (part + 1) * quarter)
        across_right[part].wait_recv()
        to_ring[3, span, :] = (rest[span] + from_ring[0, span, :].astype(F32)).astype(BF16)
        added_right[part].start()
        across_left[part].wait_recv()
        to_ring[5, span, :] = (other[span] + from_ring[1, span, :].astype(F32)).astype(BF16)
        added_left[part].start()
    along_right.wait_recv()
    along_left.wait_recv()
    lower = total[half_rows:] + from_ring[2].astype(F32)
    upper = total[:half_rows] + from_ring[4].astype(F32)
    for part in range(2):
        span = slice(part * quarter, (part + 1) * quarter)
        added_right[part].wait_recv()
        out[span, :] = (upper[span] + from_ring[3, span, :].astype(F32)).astype(BF16)
        added_left[part].wait_recv()
        out[half_rows + part * quarter:half_rows + (part + 1) * quarter, :] = (
            lower[span] + from_ring[5, span, :].astype(F32)).astype(BF16)
    shifts = across_right + across_left + added_right + added_left + [along_right, along_left]
    for copy in pairs + shifts:
        copy.wait_send()


def per_device(
    inputs, norm_gain, query_weight, key_weight, value_weight, memory_query_weight,
    memory_key_weight, memory_value_weight, input_gate_weight, forget_gate_weight, forget_bias,
    decay_shift, lambdas, head_gain, out_weight_attention, out_weight_memory,
):
    rows, columns = inputs.shape
    middle = DD // 2
    inverse = 1.0 / ROTARY_BASE ** (np.arange(middle) / middle)
    near = np.tile(np.arange(rows)[:, None] * inverse[None, :], (1, 8))
    far = np.tile((np.arange(SPANS) * rows)[:, None] * inverse[None, :], (1, 8))
    near = jnp.asarray(np.stack([np.cos(near), np.sin(near)]), F32)
    far = jnp.asarray(np.stack([np.cos(far), np.sin(far)], axis=1), F32)
    vmem = pl.BlockSpec(memory_space=pltpu.VMEM)
    anywhere = pl.BlockSpec(memory_space=pl.ANY)
    half = rows // 2
    scratch = [
        pltpu.VMEM((8, 1, columns), F32),
        pltpu.VMEM((2, rows, 128), F32),
        pltpu.VMEM((2, 128), F32),
        pltpu.VMEM((2, 2048), BF16),
        pltpu.VMEM((2, 2048), BF16),
        pltpu.SMEM((2,), F32),
        pltpu.VMEM((2, rows), F32),
        pltpu.SMEM((2,), F32),
        pltpu.VMEM((1, HEAD), F32),
        pltpu.VMEM((8, rows, columns), BF16),
        pltpu.VMEM((8, rows, columns), BF16),
        pltpu.VMEM((rows, columns), F32),
        pltpu.VMEM((3, 2048, 256), BF16),
        pltpu.VMEM((8, 256, 256), BF16),
        pltpu.VMEM((2, SPANS, rows, 128), BF16),
        pltpu.VMEM((2, 2 * rows, 128), BF16),
        pltpu.VMEM((rows, 128), BF16),
        pltpu.VMEM((rows, 128), BF16),
        pltpu.VMEM((rows, 128), BF16),
        pltpu.VMEM((2, rows, 128), F32),
        pltpu.VMEM((2, rows), F32),
        pltpu.VMEM((2, 2 * rows, 128), F32),
        pltpu.VMEM((2, 2 * rows, 128), F32),
        pltpu.VMEM((ROUNDS, HEAD + 8, 128), F32),
        pltpu.VMEM((ROUNDS, HEAD + 8, 128), F32),
        pltpu.VMEM((2, HEAD + 8, 128), F32),
        pltpu.VMEM((2, rows, 128), F32),
        pltpu.VMEM((rows, 128), F32),
        pltpu.VMEM((rows, 256), BF16),
        pltpu.VMEM((4, rows, 256), BF16),
        pltpu.VMEM((4, rows, 256), BF16),
        pltpu.VMEM((6, half, 256), BF16),
        pltpu.VMEM((6, half, 256), BF16),
        pltpu.SemaphoreType.DMA((9,)),
        pltpu.SemaphoreType.DMA((25,)),
        pltpu.SemaphoreType.DMA((13, 2)),
        pltpu.SemaphoreType.DMA((13, 2)),
        pltpu.SemaphoreType.DMA((5, 2, 4)),
        pltpu.SemaphoreType.DMA((5, 2, 4)),
        pltpu.SemaphoreType.DMA((10, 4)),
        pltpu.SemaphoreType.DMA((10, 4)),
        pltpu.SemaphoreType.DMA((ROUNDS,)),
        pltpu.SemaphoreType.DMA((ROUNDS,)),
        pltpu.SemaphoreType.DMA((4,)),
        pltpu.SemaphoreType.DMA((4,)),
        pltpu.SemaphoreType.DMA((6, 2)),
        pltpu.SemaphoreType.DMA((6, 2)),
    ]
    return pl.pallas_call(
        layer_kernel,
        out_shape=jax.ShapeDtypeStruct((rows, columns), BF16),
        in_specs=[anywhere] * 18,
        out_specs=vmem,
        scratch_shapes=scratch,
        compiler_params=pltpu.CompilerParams(
            collective_id=0, has_side_effects=True, vmem_limit_bytes=60 * 1024 * 1024),
        name="layer",
    )(
        inputs, norm_gain.reshape(8, 1, 256), near, far, query_weight, key_weight, value_weight,
        memory_query_weight, memory_key_weight, memory_value_weight, input_gate_weight.T,
        forget_gate_weight.T, forget_bias, decay_shift.T, lambdas, head_gain.reshape(1, HEAD),
        out_weight_attention, out_weight_memory,
    )


def solution(mesh):
    split = P(None, "tp")
    placed = (
        P("sp", "tp"), P(), split, split, split, split, split, split, split, split,
        P("tp"), P("sp", "tp"), P("tp"), P(), P("tp", None), P("tp", None),
    )
    return jax.shard_map(
        per_device, mesh=mesh, in_specs=placed, out_specs=P("sp", "tp"), check_vma=False)
```
